32 devices in a mesh: sp: 4 (over z), fs: 4 (over y, x), tp: 2 (over core).
Axes of the slice: x: 2, y: 2, z: 4, core: 2. Of those that a mesh axis runs over, the one named last changes fastest.
Arguments:
- inputs: bfloat16 [16384, 2048], P(('fs', 'sp'), 'tp'), parts along dimension 0, may hold values from -270 to 270
- mix_gain: float32 [2048], replicated, may hold values from 0.1 to 1.9
- w_query: bfloat16 [2048, 1024], P(None, 'tp'), may hold values from -0.125 to 0.125
- w_key: bfloat16 [2048, 256], P(None, 'tp'), may hold values from -0.125 to 0.125
- w_value: bfloat16 [2048, 256], P(None, 'tp'), may hold values from -0.125 to 0.125
- query_gain: float32 [64], replicated, may hold values from 0 to 14, as said below
- key_gain: float32 [64], replicated, may hold values from 0 to 14, as said below
- sink_logit: float32 [16], P('tp'), may hold values from 3 to 7
- w_inner: bfloat16 [2048, 1024], P(None, 'tp'), may hold values from -0.125 to 0.125
- w_bmat: bfloat16 [2048, 512], P(None, 'tp'), may hold values from -0.125 to 0.125
- w_cmat: bfloat16 [2048, 512], P(None, 'tp'), may hold values from -0.125 to 0.125
- w_gate: bfloat16 [2048, 1024], P(None, 'tp'), may hold values from -0.125 to 0.125
- w_step: bfloat16 [2048, 2, 16], P(None, None, 'tp'), may hold values from -0.125 to 0.125
- conv_inner: bfloat16 [5, 1024], P(None, 'tp'), may hold values from -2.5 to 2.5
- conv_bmat: bfloat16 [5, 512], P(None, 'tp'), may hold values from -2.5 to 2.5
- conv_cmat: bfloat16 [5, 512], P(None, 'tp'), may hold values from -2.5 to 2.5
- step_bias: float32 [2, 16], P(None, 'tp'), may hold values from -1 to 1
- decay_rate: float32 [2, 16], P(None, 'tp'), may hold values from 0 to 1, as said below
- decay_offset: float32 [4096, 2, 16], P('sp', None, 'tp'), may hold values from -3 to 0, as said below
- start_state: float32 [8, 16, 64, 128], P('fs', 'tp'), parts along dimension 0, may hold values from -96 to 96
- group_gain: float32 [1024], P('tp'), may hold values from 0.1 to 1.9
- w_out_attn: bfloat16 [1024, 2048], P('tp'), may hold values from -1.5 to 1.5
- w_out_state: bfloat16 [1024, 2048], P('tp'), may hold values from -0.1875 to 0.1875
Outputs:
- mixed: bfloat16 [16384, 2048], P(('fs', 'sp', 'tp')), parts along dimension 0
The draws below stay inside these ranges and needn't reach their ends.
There are 4 independent parts, one for each index of `fs`. The reference program is written for one: setup_inputs(seed, part) draws one part's arguments, and reference() takes and returns one part's arrays. A program takes and returns all parts, laid end to end along the dimension named above; an argument that names none is the same for every part. Nothing has to cross between parts.
Inputs may be any that keep to these rules, and one draw needn't show every extreme that they name: `query_gain`: positive. `key_gain`: positive. `decay_rate`: positive. `decay_offset`: never positive.
All inputs are finite; a program needn't handle non-finite values.
Results may differ from the reference program's by a relative error of at most 0.035.
Values may be sent and summed in bfloat16 or wider, within the bound.
A program may use at most 128 MiB of HBM per device.

```python
import math
import jax
import jax.numpy as jnp
from jax import lax

D = 2048
HEAD = 64
A_HEADS = 16
A_KV = 4
MIXER_HEADS = 16
S_GROUPS = 4
STATE = 128
CONV = 5
WINDOW = 128
STATE_BLOCK = 128
TOK_DEV = 1024
SEQUENCE_LENGTH = 4096
S_INNER = 1024
N_TP = 2


def draw_inputs(key, part):
    base_key = jax.random.fold_in(key, 11)
    noise_key, row_key, column_key = jax.random.split(base_key, 3)
    row_scale = jnp.exp(jax.random.uniform(row_key, (SEQUENCE_LENGTH, 1), jnp.float32, 0.0, math.log(10.0)))
    column_ramp = jnp.exp(math.log(4.0) * jnp.arange(D, dtype=jnp.float32) / D)
    column_scale = column_ramp[None, :] * jnp.exp(jax.random.uniform(column_key, (1, D), jnp.float32, -0.5, 0.5))
    values = jnp.clip(jax.random.normal(noise_key, (SEQUENCE_LENGTH, D), jnp.float32), -4.0, 4.0)
    return (values * row_scale * column_scale).astype(jnp.bfloat16)


def gain_table(key, salt):
    gain_key = jax.random.fold_in(key, salt)
    return jax.random.uniform(gain_key, (HEAD,), jnp.float32, 0.5, 1.5)


def draw_query_gain(key, part):
    return gain_table(key, 21)


def draw_key_gain(key, part):
    return gain_table(key, 22)


def slow_heads(key):
    ranking = jax.random.permutation(jax.random.fold_in(key, 31), 2 * MIXER_HEADS)
    kept_count = MIXER_HEADS
    return (ranking < kept_count).reshape(2, MIXER_HEADS)


def base_rates(key):
    slowly = slow_heads(key)
    quick_rates = jax.random.uniform(jax.random.fold_in(key, 41), (2, MIXER_HEADS), jnp.float32, 1.5, 2.5) / STATE_BLOCK
    return jnp.where(slowly, 0.2 / SEQUENCE_LENGTH, quick_rates)


def draw_decay_rate(key, part):
    return base_rates(key)


def draw_decay_offset(key, part):
    rates = base_rates(key)
    device_blocks = SEQUENCE_LENGTH // TOK_DEV
    factor_key, position_random_key, level_random_key = jax.random.split(jax.random.fold_in(key, 51), 3)
    factors = jnp.exp(jax.random.uniform(factor_key, (device_blocks, 1, 2, MIXER_HEADS), jnp.float32, math.log(0.5), math.log(2.5)))
    constant_level = -jnp.broadcast_to(factors * rates, (device_blocks, TOK_DEV, 2, MIXER_HEADS)).reshape(SEQUENCE_LENGTH, 2, MIXER_HEADS)
    spike_position = jax.random.randint(position_random_key, (2, 2, MIXER_HEADS), 0, SEQUENCE_LENGTH)
    spike_level = jnp.log(jax.random.uniform(level_random_key, (2, 2, MIXER_HEADS), jnp.float32, 0.5, 0.8))
    spike_mask = jnp.arange(SEQUENCE_LENGTH)[:, None, None, None] == spike_position[None]
    spike_count = jnp.sum(jnp.where(spike_mask, spike_level[None], 0.0), axis=1)
    return constant_level + spike_count


def levels(key, extent, cuts, least, high):
    loudness, own = 1.0, jax.random.fold_in(key, 6)
    for dim, shards_of in cuts:
        draws = jnp.exp(jax.random.uniform(jax.random.fold_in(own, dim), (shards_of,), jnp.float32, least / len(cuts), high / len(cuts)))
        loudness = loudness * jnp.repeat(draws, extent[dim] // shards_of).reshape([-1 if axis == dim else 1 for axis in range(len(extent))])
    return loudness


def bell_draw(stream_key, extent, scale, reach, cuts=(), kind=jnp.bfloat16):
    result = jax.random.normal(stream_key, extent, jnp.float32) * scale
    if len(cuts) > 0:
        result = levels(stream_key, extent, cuts, -0.22, 0.18) * result
    return jnp.clip(result, min=-reach, max=reach).astype(kind)


def setup_inputs(seed: int = 0, part: int = 0) -> dict:
    splits = jax.random.split(jax.random.key(seed), 24)
    own_keys = jax.random.split(jax.random.fold_in(splits[23], part), 24)
    inputs = draw_inputs(jax.random.fold_in(jax.random.fold_in(splits[23], part), 71), part)
    mix_gain = jnp.clip(1.0 + 0.18 * jax.random.normal(splits[1], (D,), jnp.float32), 0.1, 1.9)
    w_query = bell_draw(splits[2], (D, A_HEADS * HEAD), D ** -0.5, 0.125, ((1, 2),))
    w_key = bell_draw(splits[3], (D, A_KV * HEAD), D ** -0.5, 0.125, ((1, 2),))
    w_value = bell_draw(splits[4], (D, A_KV * HEAD), D ** -0.5, 0.125, ((1, 2),))
    query_gain = draw_query_gain(jax.random.fold_in(splits[23], 71), part)
    key_gain = draw_key_gain(jax.random.fold_in(splits[23], 71), part)
    sink_logit = jnp.clip(3.0 + 4.0 * jax.random.uniform(splits[7], (A_HEADS,), jnp.float32) ** levels(splits[7], (A_HEADS,), ((0, 2),), -0.2, 0.2), 3.0, 7.0)
    w_inner = bell_draw(splits[8], (D, S_INNER), D ** -0.5, 0.125, ((1, 2),))
    w_bmat = bell_draw(splits[9], (D, S_GROUPS * STATE), D ** -0.5, 0.125, ((1, 2),))
    w_cmat = bell_draw(splits[10], (D, S_GROUPS * STATE), D ** -0.5, 0.125, ((1, 2),))
    w_gate = bell_draw(splits[11], (D, S_INNER), D ** -0.5, 0.125, ((1, 2),))
    w_step = bell_draw(splits[12], (D, 2, MIXER_HEADS), D ** -0.5, 0.125, ((2, 2),))
    conv_inner = bell_draw(splits[13], (CONV, S_INNER), CONV ** -0.5, 2.5, ((1, 2),))
    conv_bmat = bell_draw(splits[14], (CONV, S_GROUPS * STATE), CONV ** -0.5, 2.5, ((1, 2),))
    conv_cmat = bell_draw(splits[15], (CONV, S_GROUPS * STATE), CONV ** -0.5, 2.5, ((1, 2),))
    step_bias = jnp.clip(jax.random.uniform(splits[16], (2, MIXER_HEADS), jnp.float32, -1.0, 1.0) * levels(splits[16], (2, MIXER_HEADS), ((1, 2),), -0.4, 0.0), -1.0, 1.0)
    decay_rate = draw_decay_rate(jax.random.fold_in(splits[23], 71), part)
    decay_offset = draw_decay_offset(jax.random.fold_in(splits[23], 71), part)
    start_state = bell_draw(own_keys[19], (2, MIXER_HEADS, HEAD, STATE), (SEQUENCE_LENGTH ** 0.5 // 4), 96.0, ((1, 2),), jnp.float32)
    group_gain = jnp.clip(1.0 + 0.18 * jax.random.normal(splits[20], (S_INNER,), jnp.float32), 0.1, 1.9)
    w_out_attn = bell_draw(splits[21], (A_HEADS * HEAD, D), (A_HEADS * HEAD // 64) ** -0.5, 1.5, ((0, 2),))
    w_out_state = bell_draw(splits[22], (S_INNER, D), S_INNER ** -0.5, 0.1875, ((0, 2),))
    return dict(inputs=inputs, mix_gain=mix_gain, w_query=w_query, w_key=w_key, w_value=w_value, query_gain=query_gain, key_gain=key_gain, sink_logit=sink_logit, w_inner=w_inner, w_bmat=w_bmat, w_cmat=w_cmat, w_gate=w_gate, w_step=w_step, conv_inner=conv_inner, conv_bmat=conv_bmat, conv_cmat=conv_cmat, step_bias=step_bias, decay_rate=decay_rate, decay_offset=decay_offset, start_state=start_state, group_gain=group_gain, w_out_attn=w_out_attn, w_out_state=w_out_state)


epsilon = 1e-06
rotary_base = 10000.0

def head_norm(values, gain):
    return values * lax.rsqrt(lax.optimization_barrier(jnp.mean(values * values, axis=-1, keepdims=True)) + epsilon) * gain

def rotate(values, positions):
    half_dim = values.shape[-1] // 2
    frequency = rotary_base ** (-jnp.arange(half_dim, dtype=jnp.float32) / half_dim)
    angles = positions.astype(jnp.float32)[:, None] * frequency[None, :]
    shaped = (angles.shape[0],) + (1,) * (values.ndim - 2) + (half_dim,)
    cosine = jnp.cos(angles).reshape(shaped)
    sine_table = jnp.sin(angles).reshape(shaped)
    first_half = values[..., :half_dim]
    second_half = values[..., half_dim:]
    return jnp.concatenate([first_half * cosine - second_half * sine_table, second_half * cosine + first_half * sine_table], axis=-1)

def attend_block(queries, keys, values, sink_logit, key_pos, length):
    scores = jnp.einsum('qhgd,khd->hgqk', queries.astype(jnp.float32), keys.astype(jnp.float32)) * HEAD ** (-0.5)
    offsets = jnp.arange(3 * WINDOW) - WINDOW
    nearby = jnp.abs(offsets[None, :] - jnp.arange(WINDOW)[:, None]) <= WINDOW
    inside = (key_pos >= 0) & (key_pos < length)
    allowed = nearby & inside[None, :]
    masked = jnp.where(allowed, scores, -jnp.inf)
    highest = jnp.maximum(lax.optimization_barrier(jnp.max(masked, axis=-1, keepdims=True)), sink_logit[:, :, None, None])
    raised = jnp.exp(masked - highest)
    denominator = jnp.exp(sink_logit[:, :, None, None] - highest) + lax.optimization_barrier(jnp.sum(raised, axis=-1, keepdims=True))
    weights = (raised / denominator).astype(jnp.bfloat16)
    return jnp.einsum('hgqk,khe->qhge', weights.astype(jnp.float32), values.astype(jnp.float32)).astype(jnp.bfloat16)

def ssd_blocks(inner_act, bmat_act, cmat_act, step_size, log_decay, carry_state):
    length = inner_act.shape[0]
    number_blocks = length // STATE_BLOCK

    def split_blocks(values):
        return values.reshape((number_blocks, STATE_BLOCK) + values.shape[1:])
    causal = jnp.arange(STATE_BLOCK)[:, None] >= jnp.arange(STATE_BLOCK)[None, :]

    def advance(running, block_data):
        inner_rows, bmat_rows, cmat_rows, step_rows, decay_rows = block_data
        cumulative = jnp.cumsum(decay_rows, axis=0)
        scores = jnp.einsum('lgn,sgn->lsg', cmat_rows.astype(jnp.float32), bmat_rows.astype(jnp.float32))
        spread = jnp.where(causal[:, :, None, None], cumulative[:, None] - cumulative[None, :], -jnp.inf)
        weights = (scores[:, :, :, None] * jnp.exp(spread) * step_rows[None]).astype(jnp.bfloat16)
        within = jnp.einsum('lsgr,sgrp->lgrp', weights.astype(jnp.float32), inner_rows.astype(jnp.float32))
        carried = jnp.einsum('lgn,grpn->lgrp', cmat_rows.astype(jnp.float32), running, precision=lax.Precision.HIGHEST) * jnp.exp(cumulative)[..., None]
        fading = jnp.exp(cumulative[-1:] - cumulative)
        loaded = (inner_rows.astype(jnp.float32) * (step_rows * fading)[..., None]).astype(jnp.bfloat16)
        running = jnp.exp(cumulative[-1])[..., None, None] * running + jnp.einsum('sgrp,sgn->grpn', loaded.astype(jnp.float32), bmat_rows.astype(jnp.float32))
        return (running, within + carried)
    final_state, outputs = lax.scan(advance, carry_state, tuple((split_blocks(values) for values in (inner_act, bmat_act, cmat_act, step_size, log_decay))))
    return (final_state, outputs.reshape((length,) + outputs.shape[2:]))

def reverse_rows(values):
    return values[::-1]

def reference(inputs, mix_gain, w_query, w_key, w_value, query_gain, key_gain, sink_logit, w_inner, w_bmat, w_cmat, w_gate, w_step, conv_inner, conv_bmat, conv_cmat, step_bias, decay_rate, decay_offset, start_state, group_gain, w_out_attn, w_out_state):
    length = inputs.shape[0]
    widened = inputs.astype(jnp.float32)
    row_scale = lax.rsqrt(lax.optimization_barrier(jnp.mean(widened * widened, axis=1, keepdims=True)) + epsilon)
    scaled_in = (widened * mix_gain).astype(jnp.bfloat16)

    def project(weight):
        return row_scale * jnp.dot(scaled_in, weight, preferred_element_type=jnp.float32)
    query_proj = project(w_query).astype(jnp.bfloat16)
    key_proj = project(w_key).astype(jnp.bfloat16)
    value_proj = project(w_value).astype(jnp.bfloat16)
    inner_proj = project(w_inner).astype(jnp.bfloat16)
    bmat_proj = project(w_bmat).astype(jnp.bfloat16)
    cmat_proj = project(w_cmat).astype(jnp.bfloat16)
    gate_proj = project(w_gate).astype(jnp.bfloat16)
    step_raw = project(w_step.reshape(D, 2 * MIXER_HEADS)).reshape(length, 2, MIXER_HEADS)
    positions = jnp.arange(length, dtype=jnp.int32)
    group_size = A_HEADS // A_KV
    query_rot = rotate(head_norm(query_proj.astype(jnp.float32).reshape(length, A_HEADS, HEAD), query_gain), positions).astype(jnp.bfloat16).reshape(length, A_KV, group_size, HEAD)
    key_rot = rotate(head_norm(key_proj.astype(jnp.float32).reshape(length, A_KV, HEAD), key_gain), positions).astype(jnp.bfloat16)
    value_rows = value_proj.reshape(length, A_KV, HEAD)
    padding = ((WINDOW, WINDOW), (0, 0), (0, 0))
    key_padded = jnp.pad(key_rot, padding)
    value_padded = jnp.pad(value_rows, padding)
    sink_table = sink_logit.reshape(A_KV, group_size)

    def one_block(block_index):
        block_start = (block_index * WINDOW).astype(jnp.int32)
        query_block = lax.dynamic_slice_in_dim(query_rot, block_start, WINDOW, 0)
        key_block = lax.dynamic_slice_in_dim(key_padded, block_start, 3 * WINDOW, 0)
        value_block = lax.dynamic_slice_in_dim(value_padded, block_start, 3 * WINDOW, 0)
        key_pos = block_start - WINDOW + jnp.arange(3 * WINDOW, dtype=jnp.int32)
        return attend_block(query_block, key_block, value_block, sink_table, key_pos, length)
    attended = lax.map(one_block, jnp.arange(length // WINDOW, dtype=jnp.int32))
    attention_out = attended.reshape(length, A_HEADS * HEAD)
    mixed_rows = jnp.concatenate([inner_proj, bmat_proj, cmat_proj], axis=1)
    conv_taps = jnp.concatenate([conv_inner, conv_bmat, conv_cmat], axis=1).astype(jnp.float32)
    rim_width = CONV // 2
    framed = jnp.pad(mixed_rows, ((rim_width, rim_width), (0, 0))).astype(jnp.float32)
    conv_sum = jnp.zeros(mixed_rows.shape, jnp.float32)
    for tap_index in range(CONV):
        conv_sum = conv_sum + framed[tap_index:tap_index + length] * conv_taps[tap_index]
    activated = jax.nn.silu(conv_sum).astype(jnp.bfloat16)
    repeats = MIXER_HEADS // S_GROUPS
    state_width = S_GROUPS * STATE
    inner_act = activated[:, :S_INNER].reshape(length, S_GROUPS, repeats, HEAD)
    bmat_act = activated[:, S_INNER:S_INNER + state_width].reshape(length, S_GROUPS, STATE)
    cmat_act = activated[:, S_INNER + state_width:].reshape(length, S_GROUPS, STATE)
    step_size = jax.nn.softplus(step_raw + step_bias)
    log_decay = -decay_rate * step_size + decay_offset

    def shaped(values):
        return values.reshape(length, S_GROUPS, repeats)
    begin_fwd = start_state[0].reshape(S_GROUPS, repeats, HEAD, STATE)
    begin_bwd = start_state[1].reshape(S_GROUPS, repeats, HEAD, STATE)
    unused_fwd, output_fwd = ssd_blocks(inner_act, bmat_act, cmat_act, shaped(step_size[:, 0]), shaped(log_decay[:, 0]), begin_fwd)
    unused_bwd, output_bwd = ssd_blocks(reverse_rows(inner_act), reverse_rows(bmat_act), reverse_rows(cmat_act), reverse_rows(shaped(step_size[:, 1])), reverse_rows(shaped(log_decay[:, 1])), begin_bwd)
    state_sum = output_fwd + reverse_rows(output_bwd)
    group_width = repeats * HEAD
    gate_rows = gate_proj.astype(jnp.float32).reshape(length, S_GROUPS, group_width)
    gated = state_sum.reshape(length, S_GROUPS, group_width) * jax.nn.silu(gate_rows)
    normed = gated * lax.rsqrt(lax.optimization_barrier(jnp.mean(gated * gated, axis=-1, keepdims=True)) + epsilon)
    state_out = (normed * group_gain.reshape(S_GROUPS, group_width)).astype(jnp.bfloat16).reshape(length, S_INNER)
    attn_cols = A_HEADS * HEAD // N_TP
    state_cols = S_INNER // N_TP
    summed = jnp.zeros((length, D), jnp.float32)
    for part_index in range(N_TP):
        partial_value = jnp.dot(attention_out[:, part_index * attn_cols:(part_index + 1) * attn_cols], w_out_attn[part_index * attn_cols:(part_index + 1) * attn_cols], preferred_element_type=jnp.float32)
        partial_value = partial_value + jnp.dot(state_out[:, part_index * state_cols:(part_index + 1) * state_cols], w_out_state[part_index * state_cols:(part_index + 1) * state_cols], preferred_element_type=jnp.float32)
        summed = summed + lax.optimization_barrier(partial_value.astype(jnp.bfloat16)).astype(jnp.float32)
    return summed.astype(jnp.bfloat16)
```

```python
import functools

import jax
import jax.numpy as jnp
import numpy as np
from jax import lax
from jax.experimental import pallas as pl
from jax.experimental.pallas import tpu as pltpu
from jax.sharding import PartitionSpec as P

HEAD = 64
STATE = 128
CONV = 5
BLK = 128
LANE = 128
ROWS = 256
EDGE = 8

epsilon = 1e-06
rotary_base = 10000.0
LOG2E = 1.4426950408889634
NEG = -1e30
F32 = jnp.float32
BF16 = jnp.bfloat16
MESH = pl.DeviceIdType.MESH


def mm(a, b):
    return jnp.dot(a, b, preferred_element_type=F32)


def mm_t(a, b):
    return lax.dot_general(a, b, (((1,), (1,)), ((), ())), preferred_element_type=F32)


def silu(v):
    return v / (1.0 + jnp.exp(-v))


def rounded(v):
    return v.astype(BF16).astype(F32)


def column(row):
    return jnp.broadcast_to(row, (LANE, LANE)).T


def pad_row(row):
    return jnp.concatenate([row, jnp.zeros((1, LANE - row.shape[1]), F32)], axis=1)


def pieces(v):
    hi = v.astype(BF16)
    rest = v - hi.astype(F32)
    mid = rest.astype(BF16)
    lo = (rest - mid.astype(F32)).astype(BF16)
    return hi, mid, lo


def kernel(
    x_hbm, wq, wk, wv, wi, wb, wc, wg, woa, wos,
    ws, mix_gain, qgain1, kgain1, sink, taps_i, taps_b, taps_c, bias2, rate2, offs, start, ggain,
    cos_t, sin_t, cos_o, sin_o, tri,
    out_hbm,
    w, wsp, wo, xown, xpeer, xs, rs, rot, kn, vt, xb, qt, gt, bc, xt, st, ct, dec, ld, ggt, bias_m,
    gs, agg, dtot, sb, z, psend, precv, outv, xhalo, chain_s, chain_r,
    sem_w, sem_x, sem_xs, sem_xr, sem_hs, sem_hr, sem_cs, sem_cr, sem_ps, sem_pr, sem_o,
    *, n_sp,
):
    me = lax.axis_index("tp")
    idx = lax.axis_index("sp")
    peer = 1 - me
    T, half = x_hbm.shape
    nb = T // BLK
    nchunk = T // ROWS
    per = ROWS // BLK
    has_prev = idx > 0
    has_next = idx < n_sp - 1

    barrier = pltpu.get_barrier_semaphore()
    pl.semaphore_signal(barrier, inc=1, device_id={"tp": peer}, device_id_type=MESH)

    @pl.when(has_prev)
    def _():
        pl.semaphore_signal(barrier, inc=1, device_id={"sp": idx - 1}, device_id_type=MESH)

    @pl.when(has_next)
    def _():
        pl.semaphore_signal(barrier, inc=1, device_id={"sp": idx + 1}, device_id_type=MESH)

    own_copies = []
    for i in range(nchunk):
        c = pltpu.make_async_copy(
            x_hbm.at[pl.ds(i * ROWS, ROWS)], xown.at[pl.ds(i * ROWS, ROWS)], sem_x.at[i]
        )
        c.start()
        own_copies.append(c)
    wcopies = []
    col = 0
    for j, src in enumerate((wi, wb, wc, wk, wv, wq, wg)):
        width = src.shape[1]
        c = pltpu.make_async_copy(src, w.at[:, pl.ds(col, width)], sem_w.at[j])
        c.start()
        wcopies.append(c)
        col += width
    n_w = len(wcopies)
    na = woa.shape[0]
    oc = [
        pltpu.make_async_copy(woa, wo.at[pl.ds(0, na)], sem_w.at[n_w]),
        pltpu.make_async_copy(wos, wo.at[pl.ds(na, wos.shape[0])], sem_w.at[n_w + 1]),
    ]
    for c in oc:
        c.start()

    inner_w = wi.shape[1]
    state_w = wb.shape[1]
    xw = inner_w + 2 * state_w
    kvw = wk.shape[1]
    qw = wq.shape[1]
    gw = wg.shape[1]
    kvcol = xw
    qcol = xw + 2 * kvw
    gcol = qcol + qw
    hd2 = ws.shape[0]
    heads = hd2 // 2
    groups = state_w // STATE
    per_group = heads // groups
    gwid = per_group * HEAD
    kv_heads = kvw // HEAD
    q_per = (qw // HEAD) // kv_heads
    sq = (BLK, BLK)
    ri = lax.broadcasted_iota(jnp.int32, sq, 0)
    ci = lax.broadcasted_iota(jnp.int32, sq, 1)

    wsp[hd2:, :] = jnp.zeros((LANE - hd2, wsp.shape[1]), BF16)
    wsp[0:hd2, :] = ws[...]
    qt[...] = jnp.zeros_like(qt)
    agg[...] = jnp.zeros_like(agg)
    qg = column(pad_row(qgain1[...] * (HEAD ** (-0.5) * LOG2E)))
    kg = column(pad_row(kgain1[...]))
    hh = HEAD // 2
    co = cos_o[idx]
    so = sin_o[idx]
    for b in range(nb):
        cols = slice(b * BLK, (b + 1) * BLK)
        c0 = cos_t[:, cols]
        s0 = sin_t[:, cols]
        cosine = co * c0 - so * s0
        sine = so * c0 + co * s0
        for k, gain in enumerate((qg, kg)):
            ga, gb = gain[0:hh], gain[hh:HEAD]
            rot[k, b, 0:hh] = ga * cosine
            rot[k, b, hh : 2 * hh] = gb * sine
            rot[k, b, 2 * hh : 3 * hh] = gb * cosine
            rot[k, b, 3 * hh : 4 * hh] = ga * sine
    bias = column(pad_row(jnp.concatenate([bias2[0:1, :], bias2[1:2, :]], axis=1)))[0:hd2]
    rate = column(pad_row(jnp.concatenate([rate2[0:1, :], rate2[1:2, :]], axis=1)))[0:hd2]
    for s in range(0, inner_w, LANE):
        ggt[s : s + LANE, :] = column(ggain[:, s : s + LANE])
    bias_m[0] = jnp.where(ri >= ci, 0.0, NEG)
    bias_m[1] = jnp.where(ri <= ci, 0.0, NEG)

    @pl.when(has_prev & has_next)
    def _():
        pl.semaphore_wait(barrier, 3)

    @pl.when(jnp.logical_not(has_prev & has_next))
    def _():
        pl.semaphore_wait(barrier, 2 if n_sp > 1 else 1)

    gath = []
    for i in range(nchunk):
        c = pltpu.make_async_remote_copy(
            src_ref=x_hbm.at[pl.ds(i * ROWS, ROWS)],
            dst_ref=xpeer.at[pl.ds(i * ROWS, ROWS)],
            send_sem=sem_xs.at[i],
            recv_sem=sem_xr.at[i],
            device_id={"tp": peer},
            device_id_type=MESH,
        )
        c.start()
        gath.append(c)

    gain_own = mix_gain[:, pl.ds(pl.multiple_of(me * half, LANE), half)]
    gain_peer = mix_gain[:, pl.ds(pl.multiple_of(peer * half, LANE), half)]

    def scale_half(i, src, gain, base, add):
        dst = pl.multiple_of(base * half, LANE)

        def body(r, carry):
            rows = pl.ds(pl.multiple_of(i * ROWS + r * 32, 32), 32)
            total = rs[rows, :] if add else jnp.zeros((32, LANE), F32)
            for s in range(0, half, LANE):
                a = src[rows, s : s + LANE].astype(F32)
                total = total + a * a
                xs[rows, pl.ds(pl.multiple_of(dst + s, LANE), LANE)] = (
                    a * gain[:, s : s + LANE]
                ).astype(BF16)
            rs[rows, :] = total
            return carry

        lax.fori_loop(0, ROWS // 32, body, 0, unroll=2)

    def finish_scale(i):
        rows = slice(i * ROWS, (i + 1) * ROWS)
        total = jnp.sum(rs[rows, :], axis=1, keepdims=True)
        rs[rows, :] = jnp.broadcast_to(
            lax.rsqrt(total * (1.0 / (2 * half)) + epsilon), (ROWS, LANE)
        )

    for i in range(nchunk):
        own_copies[i].wait()
        scale_half(i, xown, gain_own, me, False)
    for i in range(nchunk):
        gath[i].wait()
        scale_half(i, xpeer, gain_peer, peer, True)
        finish_scale(i)

    def row_chunk(i):
        start_row = pl.multiple_of(i * ROWS, ROWS)
        return start_row, pl.ds(start_row, ROWS)

    def norm_rotate(v, k, b):
        inv = lax.rsqrt(jnp.sum(v * v, axis=0, keepdims=True) * (1.0 / HEAD) + epsilon)
        a, c = v[0:hh], v[hh:HEAD]
        first = (a * rot[k, b, 0:hh] - c * rot[k, b, hh : 2 * hh]) * inv
        second = (c * rot[k, b, 2 * hh : 3 * hh] + a * rot[k, b, 3 * hh : 4 * hh]) * inv
        return jnp.concatenate([first, second], axis=0)

    def remote(src, dst, ss, rsem, target):
        return pltpu.make_async_remote_copy(
            src_ref=src, dst_ref=dst, send_sem=ss, recv_sem=rsem,
            device_id={"sp": target}, device_id_type=MESH,
        )

    for j in (0, 1, 2):
        wcopies[j].wait()

    def x_step(i, carry):
        r0, rows = row_chunk(i)
        scale = rs[rows, :]
        xr = xs[rows, :]
        dst = pl.ds(pl.multiple_of(r0 + EDGE, EDGE), ROWS)
        for s in range(0, xw, 256):
            p = mm(xr, w[:, s : s + 256])
            for t in range(0, 256, LANE):
                xb[(s + t) // LANE, dst, :] = rounded(p[:, t : t + LANE] * scale)
        p = mm_t(xr, wsp[...]) * scale
        pt = p.T[0:hd2]
        for u in range(per):
            b = i * per + u
            v = pt[:, u * BLK : (u + 1) * BLK] + bias
            step = jnp.maximum(v, 0.0) + jnp.log1p(jnp.exp(-jnp.abs(v)))
            st[b] = step
            ld[b] = -rate * step + offs[:, pl.ds(pl.multiple_of(b * BLK, BLK), BLK)]
        return carry

    lax.fori_loop(0, nchunk, x_step, 0)

    x_up = remote(xb.at[:, pl.ds(T, EDGE)], xhalo.at[0], sem_hs.at[2], sem_hr.at[2], idx + 1)
    x_dn = remote(xb.at[:, pl.ds(EDGE, EDGE)], xhalo.at[1], sem_hs.at[3], sem_hr.at[3], idx - 1)
    k_up = remote(kn.at[pl.ds(T, BLK)], kn.at[pl.ds(0, BLK)], sem_hs.at[0], sem_hr.at[0], idx + 1)
    k_dn = remote(kn.at[pl.ds(BLK, BLK)], kn.at[pl.ds(T + BLK, BLK)], sem_hs.at[1], sem_hr.at[1], idx - 1)
    v_up = remote(vt.at[:, pl.ds(T, BLK)], vt.at[:, pl.ds(0, BLK)], sem_hs.at[4], sem_hr.at[4], idx + 1)
    v_dn = remote(vt.at[:, pl.ds(BLK, BLK)], vt.at[:, pl.ds(T + BLK, BLK)], sem_hs.at[5], sem_hr.at[5], idx - 1)

    @pl.when(has_next)
    def _():
        x_up.start()

    @pl.when(has_prev)
    def _():
        x_dn.start()

    wcopies[3].wait()
    wcopies[4].wait()

    def kv_step(i, carry):
        r0, rows = row_chunk(i)
        p = mm(xs[rows, :], w[:, kvcol : kvcol + 2 * kvw])
        scale = rs[rows, :]
        for u in range(per):
            b = i * per + u
            part = slice(u * BLK, (u + 1) * BLK)
            kt = rounded(p[part, :LANE] * scale[part]).T
            kt = jnp.concatenate(
                [norm_rotate(kt[h * HEAD : (h + 1) * HEAD], 1, b) for h in range(kv_heads)], axis=0
            )
            dst = pl.multiple_of(r0 + (u + 1) * BLK, BLK)
            kn[pl.ds(dst, BLK), :] = kt.T.astype(BF16)
            vt[:, pl.ds(dst, BLK)] = (p[part, LANE:] * scale[part]).T.astype(BF16)
        return carry

    lax.fori_loop(0, nchunk, kv_step, 0)

    @pl.when(has_next)
    def _():
        k_up.start()
        v_up.start()

    @pl.when(has_prev)
    def _():
        k_dn.start()
        v_dn.start()

    lhs = []
    for b in range(nb):
        lhs += list(pieces(ld[b]))
    sums = mm(jnp.concatenate(lhs, axis=0), tri[...])
    last_f = last_b = None
    for b in range(nb):
        tot = sums[3 * b * hd2 : (3 * b + 1) * hd2]
        tot = tot + sums[(3 * b + 1) * hd2 : (3 * b + 2) * hd2]
        tot = (tot + sums[(3 * b + 2) * hd2 : (3 * b + 3) * hd2]) * LOG2E
        c = jnp.concatenate([tot[0:heads, 0:BLK], tot[heads:, BLK:]], axis=0)
        ct[b] = c
        end = jnp.concatenate(
            [
                jnp.broadcast_to(c[0:heads, BLK - 1 : BLK], (heads, BLK)),
                jnp.broadcast_to(c[heads:, 0:1], (heads, BLK)),
            ],
            axis=0,
        )
        dec[b] = jnp.exp2(end)
        ld[b] = st[b] * jnp.exp2(end - c)
        total = end if b == 0 else total + end
        if b < nb - 1:
            dtot[1 + b] = jnp.exp2(total)
    dtot[0] = jnp.exp2(total)

    @pl.when(has_next)
    def _():
        x_up.wait_send()
        x_dn.wait_recv()
        xb[:, pl.ds(T + EDGE, EDGE), :] = xhalo[1]

    @pl.when(jnp.logical_not(has_next))
    def _():
        xb[:, pl.ds(T + EDGE, EDGE), :] = jnp.zeros((xb.shape[0], EDGE, LANE), F32)

    @pl.when(has_prev)
    def _():
        x_dn.wait_send()
        x_up.wait_recv()
        xb[:, pl.ds(0, EDGE), :] = xhalo[0]

    @pl.when(jnp.logical_not(has_prev))
    def _():
        xb[:, pl.ds(0, EDGE), :] = jnp.zeros((xb.shape[0], EDGE, LANE), F32)

    def spread(values, row, n):
        return jnp.broadcast_to(values[row : row + 1, :], (n, LANE))

    def state_step(b, carry):
        rows = pl.ds(pl.multiple_of(b * BLK, BLK), BLK)
        load = ld[b]
        before = jnp.where(b == 0, jnp.ones((hd2, LANE), F32), dtot[b])
        dc = dec[b]
        for tile in list(range(inner_w // LANE, xw // LANE)) + list(range(inner_w // LANE)):
            s = tile * LANE
            if s < inner_w:
                tap = taps_i[:, s : s + LANE].astype(F32)
            elif s < inner_w + state_w:
                tap = taps_b[:, s - inner_w : s - inner_w + LANE].astype(F32)
            else:
                o = s - inner_w - state_w
                tap = taps_c[:, o : o + LANE].astype(F32)
            acc = None
            for j in range(CONV):
                win = xb[tile, pl.ds(b * BLK + (EDGE - CONV // 2 + j), BLK), :]
                term = win * tap[j : j + 1]
                acc = term if acc is None else acc + term
            a = silu(acc)
            if s >= inner_w:
                bc[rows, s - inner_w : s - inner_w + LANE] = a.astype(BF16)
                continue
            at = rounded(a.T)
            xt[b, s : s + LANE, :] = at.astype(BF16)
            g = s // gwid
            bm = bc[rows, g * STATE : (g + 1) * STATE]
            loaded = []
            for direction in range(2):
                for u in range(LANE // HEAD):
                    h = tile * (LANE // HEAD) + u
                    loaded.append(
                        (at[u * HEAD : (u + 1) * HEAD] * spread(load, direction * heads + h, HEAD)).astype(BF16)
                    )
            gsum = mm(jnp.concatenate(loaded, axis=0), bm)
            for direction in range(2):
                part = gsum[direction * LANE : (direction + 1) * LANE]
                gs[b, direction, s : s + LANE, :] = part
                old = agg[direction, s : s + LANE, :]
                for u in range(LANE // HEAD):
                    h = tile * (LANE // HEAD) + u
                    sl = slice(u * HEAD, (u + 1) * HEAD)
                    if direction == 0:
                        new = old[sl] * spread(dc, h, HEAD) + part[sl]
                    else:
                        new = old[sl] + part[sl] * spread(before, heads + h, HEAD)
                    agg[direction, s + u * HEAD : s + (u + 1) * HEAD, :] = new
        return carry

    lax.fori_loop(0, nb, state_step, 0)

    hops = [
        [
            remote(
                chain_s.at[d, pl.ds(g * gwid, gwid)], chain_r.at[d, pl.ds(g * gwid, gwid)],
                sem_cs.at[d * groups + g], sem_cr.at[d * groups + g],
                idx + 1 if d == 0 else idx - 1,
            )
            for g in range(groups)
        ]
        for d in range(2)
    ]
    sources = (has_prev, has_next)
    targets = (has_next, has_prev)
    order_of = (idx, n_sp - 1 - idx)

    def hop(direction, inner):
        for g in range(groups):
            if inner:
                hops[direction][g].wait_recv()
            for u in range(per_group):
                h = g * per_group + u
                rows = slice(h * HEAD, (h + 1) * HEAD)
                enter = chain_r[direction, rows, :].astype(F32) if inner else start[direction, rows, :]
                out = enter * spread(dtot[0], direction * heads + h, HEAD) + agg[direction, rows, :]
                chain_s[direction, rows, :] = out.astype(BF16)
            hops[direction][g].start()

    for d in range(2):
        @pl.when(targets[d] & jnp.logical_not(sources[d]))
        def _(d=d):
            hop(d, False)

    slots = nchunk + nb

    def maybe_hop(slot):
        for d in range(2):
            turn = (order_of[d] * slots) // max(n_sp - 1, 1)

            @pl.when((slot == turn) & targets[d] & sources[d])
            def _(d=d):
                hop(d, True)

    wcopies[5].wait()
    wcopies[6].wait()

    def q_step(i, carry):
        maybe_hop(i)
        r0, rows = row_chunk(i)
        scale = rs[rows, :]
        xr = xs[rows, :]
        for s in range(0, qw, 256):
            p = mm(xr, w[:, qcol + s : qcol + s + 256])
            for u in range(per):
                b = i * per + u
                part = slice(u * BLK, (u + 1) * BLK)
                for t in range(0, 256, LANE):
                    q = rounded(p[part, t : t + LANE] * scale[part]).T
                    for v in range(LANE // HEAD):
                        h = (s + t) // HEAD + v
                        g = h // q_per
                        qt[b, g * HEAD : (g + 1) * HEAD, h * BLK : (h + 1) * BLK] = norm_rotate(
                            q[v * HEAD : (v + 1) * HEAD], 0, b
                        ).astype(BF16)
        for s in range(0, gw, 256):
            p = mm(xr, w[:, gcol + s : gcol + s + 256])
            for u in range(per):
                b = i * per + u
                part = slice(u * BLK, (u + 1) * BLK)
                for t in range(0, 256, LANE):
                    gate = rounded(p[part, t : t + LANE] * scale[part]).T
                    gt[b, s + t : s + t + LANE, :] = silu(gate)
        return carry

    lax.fori_loop(0, nchunk, q_step, 0)

    @pl.when(has_next)
    def _():
        k_up.wait_send()
        v_up.wait_send()
        k_dn.wait_recv()
        v_dn.wait_recv()

    @pl.when(jnp.logical_not(has_next))
    def _():
        kn[pl.ds(T + BLK, BLK), :] = jnp.zeros((BLK, kvw), BF16)
        vt[:, pl.ds(T + BLK, BLK)] = jnp.zeros((kvw, BLK), BF16)

    @pl.when(has_prev)
    def _():
        k_dn.wait_send()
        v_dn.wait_send()
        k_up.wait_recv()
        v_up.wait_recv()

    @pl.when(jnp.logical_not(has_prev))
    def _():
        kn[pl.ds(0, BLK), :] = jnp.zeros((BLK, kvw), BF16)
        vt[:, pl.ds(0, BLK)] = jnp.zeros((kvw, BLK), BF16)

    key_w = 3 * BLK
    ones = jnp.ones((16, key_w), BF16)
    sinks = sink[...] * LOG2E

    def attend(b, carry):
        maybe_hop(nchunk + b)
        rows = pl.ds(pl.multiple_of(b * BLK, BLK), BLK)
        span = pl.ds(pl.multiple_of(b * BLK, BLK), key_w)
        keys = kn[span, :]
        lo = bias_m[0] + jnp.where((idx == 0) & (b == 0), NEG, 0.0)
        hi = bias_m[1] + jnp.where((idx == n_sp - 1) & (b == nb - 1), NEG, 0.0)
        for pair in range(qw // HEAD // 2):
            g = 2 * pair // q_per
            vals = jnp.concatenate([vt[g * HEAD : (g + 1) * HEAD, span], ones], axis=0)
            s_all = mm(keys, qt[b, :, 2 * pair * BLK : 2 * (pair + 1) * BLK])
            probs, adds = [], []
            for u in range(2):
                h = 2 * pair + u
                s = s_all[:, u * BLK : (u + 1) * BLK]
                s = jnp.concatenate([s[0:BLK] + lo, s[BLK : 2 * BLK], s[2 * BLK :] + hi], axis=0)
                sk = jnp.broadcast_to(sinks[:, h : h + 1], (1, BLK))
                m = jnp.maximum(jnp.max(s, axis=0, keepdims=True), sk)
                probs.append(jnp.exp2(s - m).astype(BF16))
                adds.append(jnp.exp2(sk - m))
            o = mm(vals, jnp.concatenate(probs, axis=1))
            outs = []
            for u in range(2):
                cols = slice(u * BLK, (u + 1) * BLK)
                inv = 1.0 / (o[HEAD : HEAD + 1, cols] + adds[u])
                outs.append(o[0:HEAD, cols] * inv)
            z[rows, pair * LANE : (pair + 1) * LANE] = jnp.concatenate(outs, axis=0).T.astype(BF16)
        return carry

    lax.fori_loop(0, nb, attend, 0)

    for d in range(2):
        @pl.when(targets[d])
        def _(d=d):
            for c in hops[d]:
                c.wait_send()

        @pl.when(sources[d] & jnp.logical_not(targets[d]))
        def _(d=d):
            for c in hops[d]:
                c.wait_recv()

    for d in range(2):
        order = list(range(nb)) if d == 0 else list(range(nb - 1, -1, -1))
        for h in range(heads):
            rows = slice(h * HEAD, (h + 1) * HEAD)
            total = jnp.where(sources[d], chain_r[d, rows, :].astype(F32), start[d, rows, :])
            for b in order:
                sb[b, d, rows, :] = total.astype(BF16)
                if b != order[-1]:
                    total = total * spread(dec[b], d * heads + h, HEAD) + gs[b, d, rows, :]

    attn_w = qw
    zero_pad = jnp.zeros((LANE - hd2, LANE), F32)

    def mix_block(b):
        rows = pl.ds(pl.multiple_of(b * BLK, BLK), BLK)
        c = ct[b]
        step = st[b]
        e = c - jnp.log2(jnp.maximum(step, 1e-37))
        en = jnp.concatenate([e, zero_pad], axis=0).T
        both = jnp.log2(jnp.maximum(step[0:heads] + step[heads:], 1e-37))
        grow = jnp.exp2(c)
        before = ri < ci
        same = ri == ci
        for g in range(groups):
            bm = bc[rows, g * STATE : (g + 1) * STATE]
            cm = bc[rows, state_w + g * STATE : state_w + (g + 1) * STATE]
            scores = mm_t(bm, cm)
            states = jnp.concatenate(
                [sb[b, d, g * gwid : (g + 1) * gwid, :] for d in range(2)], axis=0
            )
            carried = mm_t(states, cm)
            gated = []
            for u in range(per_group):
                h = g * per_group + u
                arg = jnp.where(
                    before,
                    spread(c, h, BLK) - jnp.broadcast_to(en[:, h : h + 1], sq),
                    spread(c, heads + h, BLK) - jnp.broadcast_to(en[:, heads + h : heads + h + 1], sq),
                )
                arg = jnp.where(same, spread(both, h, BLK), arg)
                weights = (scores * jnp.exp2(arg)).astype(BF16)
                y = mm(xt[b, h * HEAD : (h + 1) * HEAD, :], weights)
                y = y + carried[u * HEAD : (u + 1) * HEAD] * spread(grow, h, HEAD)
                y = y + carried[gwid + u * HEAD : gwid + (u + 1) * HEAD] * spread(grow, heads + h, HEAD)
                gated.append(y * gt[b, h * HEAD : (h + 1) * HEAD, :])
            total = sum(jnp.sum(v * v, axis=0, keepdims=True) for v in gated)
            inv = lax.rsqrt(total * (1.0 / gwid) + epsilon)
            for t in range(per_group // 2):
                s = g * gwid + t * LANE
                v = jnp.concatenate([gated[2 * t], gated[2 * t + 1]], axis=0)
                z[rows, attn_w + s : attn_w + s + LANE] = (v * inv * ggt[s : s + LANE, :]).T.astype(BF16)

    for c in oc:
        c.wait()
    half_rows = T // 2
    steps = half_rows // ROWS
    width = wo.shape[1]

    def mix_rows(base):
        def one(k, carry):
            mix_block(base // BLK + k)
            return carry

        lax.fori_loop(0, ROWS // BLK, one, 0, unroll=True)

    copies = [
        pltpu.make_async_remote_copy(
            src_ref=psend.at[pl.ds(i * ROWS, ROWS)],
            dst_ref=precv.at[pl.ds(i * ROWS, ROWS)],
            send_sem=sem_ps.at[i],
            recv_sem=sem_pr.at[i],
            device_id={"tp": peer},
            device_id_type=MESH,
        )
        for i in range(steps)
    ]
    outs = [
        pltpu.make_async_copy(
            outv.at[pl.ds(i * ROWS, ROWS)], out_hbm.at[pl.ds(i * ROWS, ROWS)], sem_o.at[i]
        )
        for i in range(steps)
    ]
    for i in range(steps):
        base = peer * half_rows + i * ROWS
        mix_rows(base)
        zr = z[pl.ds(pl.multiple_of(base, ROWS), ROWS), :]
        for s in range(0, width, 512):
            psend[i * ROWS : (i + 1) * ROWS, s : s + 512] = mm(zr, wo[:, s : s + 512]).astype(BF16)
        copies[i].start()
    for i in range(steps):
        base = me * half_rows + i * ROWS
        mix_rows(base)
        zr = z[pl.ds(pl.multiple_of(base, ROWS), ROWS), :]
        for s in range(0, width, 512):
            part = rounded(mm(zr, wo[:, s : s + 512]))
            if s == 0:
                copies[i].wait()
            got = precv[i * ROWS : (i + 1) * ROWS, s : s + 512].astype(F32)
            outv[i * ROWS : (i + 1) * ROWS, s : s + 512] = (part + got).astype(BF16)
        outs[i].start()
    for c in outs:
        c.wait()


def tables(tokens, count):
    half = HEAD // 2
    frequency = rotary_base ** (-np.arange(half, dtype=np.float64) / half)
    inner = frequency[:, None] * np.arange(tokens, dtype=np.float64)[None, :]
    outer = np.arange(count, dtype=np.float64)[:, None] * tokens * frequency[None, :]
    outer = np.broadcast_to(outer[:, :, None], (count, half, LANE))
    return [f(a).astype(np.float32) for a in (inner, outer) for f in (np.cos, np.sin)]


def local(
    n_sp,
    inputs, mix_gain, w_query, w_key, w_value, query_gain, key_gain, sink_logit,
    w_inner, w_bmat, w_cmat, w_gate, w_step, conv_inner, conv_bmat, conv_cmat,
    step_bias, decay_rate, decay_offset, start_state, group_gain, w_out_attn, w_out_state,
):
    T, half = inputs.shape
    depth = w_query.shape[0]
    heads = w_step.shape[2]
    inner_w = w_inner.shape[1]
    state_w = w_bmat.shape[1]
    xw = inner_w + 2 * state_w
    kvw = w_key.shape[1]
    qw = w_query.shape[1]
    gw = w_gate.shape[1]
    width = w_out_attn.shape[1]
    nb = T // BLK
    nchunk = T // ROWS
    groups = state_w // STATE

    ws = jnp.transpose(w_step, (1, 2, 0)).reshape(2 * heads, depth)
    offs = jnp.transpose(decay_offset, (1, 2, 0)).reshape(2 * heads, T)
    start = start_state.reshape(2, inner_w, STATE)
    ct, sn, co, so = tables(T, n_sp)
    tri = np.triu(np.ones((BLK, BLK), np.float32))
    tri = np.concatenate([tri, tri.T], axis=1)
    any_spec = pl.BlockSpec(memory_space=pl.ANY)
    vm = pl.BlockSpec(memory_space=pltpu.VMEM)
    wcols = 2 * kvw + xw + qw + gw
    V = pltpu.VMEM
    dma = pltpu.SemaphoreType.DMA
    steps = T // 2 // ROWS
    hd2 = 2 * heads
    scratch = [
        V((depth, wcols), BF16), V((LANE, depth), BF16),
        V((w_out_attn.shape[0] + w_out_state.shape[0], width), BF16),
        V((T, half), BF16), V((T, half), BF16), V((T, 2 * half), BF16), V((T, LANE), F32),
        V((2, nb, 2 * HEAD, LANE), F32),
        V((T + 2 * BLK, kvw), BF16), V((kvw, T + 2 * BLK), BF16),
        V((xw // LANE, T + 2 * EDGE, LANE), F32),
        V((nb, kvw, qw // HEAD * BLK), BF16), V((nb, gw, BLK), F32),
        V((T, 2 * state_w), BF16), V((nb, inner_w, BLK), BF16),
        V((nb, hd2, BLK), F32), V((nb, hd2, BLK), F32), V((nb, hd2, BLK), F32), V((nb, hd2, BLK), F32),
        V((inner_w, LANE), F32), V((2, BLK, BLK), F32),
        V((nb, 2, inner_w, STATE), F32), V((2, inner_w, STATE), F32), V((nb, hd2, LANE), F32),
        V((nb, 2, inner_w, STATE), BF16),
        V((T, qw + inner_w), BF16),
        V((T // 2, width), BF16), V((T // 2, width), BF16), V((T // 2, width), BF16),
        V((2, xw // LANE, EDGE, LANE), F32),
        V((2, inner_w, STATE), BF16), V((2, inner_w, STATE), BF16),
        dma((9,)), dma((nchunk,)), dma((nchunk,)), dma((nchunk,)),
        dma((6,)), dma((6,)), dma((2 * groups,)), dma((2 * groups,)), dma((steps,)), dma((steps,)),
        dma((steps,)),
    ]
    return pl.pallas_call(
        functools.partial(kernel, n_sp=n_sp),
        out_shape=jax.ShapeDtypeStruct((T // 2, width), BF16),
        in_specs=[any_spec] * 10 + [vm] * 18,
        out_specs=any_spec,
        scratch_shapes=scratch,
        compiler_params=pltpu.CompilerParams(
            collective_id=0, has_side_effects=True, vmem_limit_bytes=67043328
        ),
        name="mixer",
    )(
        inputs, w_query, w_key, w_value, w_inner, w_bmat, w_cmat, w_gate,
        w_out_attn, w_out_state, ws,
        mix_gain.reshape(1, -1), query_gain.reshape(1, -1), key_gain.reshape(1, -1),
        sink_logit.reshape(1, -1), conv_inner, conv_bmat, conv_cmat, step_bias, decay_rate,
        offs, start,
        group_gain.reshape(1, -1), jnp.asarray(ct), jnp.asarray(sn), jnp.asarray(co),
        jnp.asarray(so), jnp.asarray(tri).astype(BF16),
    )


def solution(mesh):
    return jax.shard_map(
        functools.partial(local, mesh.shape["sp"]),
        mesh=mesh,
        in_specs=(
            P(("fs", "sp"), "tp"),
            P(),
            P(None, "tp"),
            P(None, "tp"),
            P(None, "tp"),
            P(),
            P(),
            P("tp"),
            P(None, "tp"),
            P(None, "tp"),
            P(None, "tp"),
            P(None, "tp"),
            P(None, None, "tp"),
            P(None, "tp"),
            P(None, "tp"),
            P(None, "tp"),
            P(None, "tp"),
            P(None, "tp"),
            P("sp", None, "tp"),
            P("fs", "tp", None, None),
            P("tp"),
            P("tp", None),
            P("tp", None),
        ),
        out_specs=P(("fs", "sp", "tp"), None),
        check_vma=False,
    )
```

```python
import functools

import jax
import jax.numpy as jnp
import numpy as np
from jax import lax
from jax.experimental import pallas as pl
from jax.experimental.pallas import tpu as pltpu
from jax.sharding import PartitionSpec as P

HEAD = 64
STATE = 128
CONV = 5
BLK = 128
LANE = 128
ROWS = 256
EDGE = 8

epsilon = 1e-06
rotary_base = 10000.0
LOG2E = 1.4426950408889634
NEG = -1e30
F32 = jnp.float32
BF16 = jnp.bfloat16
MESH = pl.DeviceIdType.MESH


def mm(a, b):
    return jnp.dot(a, b, preferred_element_type=F32)


def mm_t(a, b):
    return lax.dot_general(a, b, (((1,), (1,)), ((), ())), preferred_element_type=F32)


def silu(v):
    return v / (1.0 + jnp.exp(-v))


def rounded(v):
    return v.astype(BF16).astype(F32)


def column(row):
    return jnp.broadcast_to(row, (LANE, LANE)).T


def pad_row(row):
    return jnp.concatenate([row, jnp.zeros((1, LANE - row.shape[1]), F32)], axis=1)


def pieces(v):
    hi = v.astype(BF16)
    rest = v - hi.astype(F32)
    mid = rest.astype(BF16)
    lo = (rest - mid.astype(F32)).astype(BF16)
    return hi, mid, lo


def interleave(main, hosted):
    main = list(main)
    hosted = list(hosted)
    done = 0
    for i, step in enumerate(main):
        want = ((i + 1) * len(hosted)) // len(main)
        step()
        while done < want:
            hosted[done]()
            done += 1


def kernel(
    x_hbm, wq, wk, wv, wi, wb, wc, wg, woa, wos, start_hbm,
    ws_h, mix_gain_h, qgain_h, kgain_h, sink_h, taps_i_h, taps_b_h, taps_c_h, bias_h, rate_h, offs_h,
    ggain_h, cos_t_h, sin_t_h, cos_o_h, sin_o_h, tri_h,
    outv,
    ws, mix_gain, qgain1, kgain1, sink, taps_i, taps_b, taps_c, bias2, rate2, offs,
    ggain, cos_t, sin_t, cos_o, sin_o, tri,
    w, wsp, wo, start, xown, xpeer, xs, rs, rot, kn, vt, xb, qt, gt, bc, xt, st, ct, dec, ld, ggt, bias_m,
    gs, agg, dtot, sb, z, psend, precv, xhalo, chain_s, chain_r,
    sem_v, sem_w, sem_x, sem_xs, sem_xr, sem_hs, sem_hr, sem_cs, sem_cr, sem_ps, sem_pr,
    *, n_sp,
):
    me = lax.axis_index("tp")
    idx = lax.axis_index("sp")
    peer = 1 - me
    T, half = x_hbm.shape
    nb = T // BLK
    nchunk = T // ROWS
    per = ROWS // BLK
    has_prev = idx > 0
    has_next = idx < n_sp - 1

    own_copies = []
    for i in range(nchunk):
        c = pltpu.make_async_copy(
            x_hbm.at[pl.ds(i * ROWS, ROWS)], xown.at[pl.ds(i * ROWS, ROWS)], sem_x.at[i]
        )
        c.start()
        own_copies.append(c)

    barrier = pltpu.get_barrier_semaphore()
    pl.semaphore_signal(barrier, inc=1, device_id={"tp": peer}, device_id_type=MESH)

    @pl.when(has_prev)
    def _():
        pl.semaphore_signal(barrier, inc=1, device_id={"sp": idx - 1}, device_id_type=MESH)

    @pl.when(has_next)
    def _():
        pl.semaphore_signal(barrier, inc=1, device_id={"sp": idx + 1}, device_id_type=MESH)

    small = []
    for j, (src, dst) in enumerate((
        (mix_gain_h, mix_gain), (qgain_h, qgain1), (kgain_h, kgain1), (cos_o_h, cos_o), (sin_o_h, sin_o),
        (cos_t_h, cos_t), (sin_t_h, sin_t), (bias_h, bias2), (rate_h, rate2), (ggain_h, ggain), (ws_h, ws),
        (sink_h, sink), (taps_i_h, taps_i), (taps_b_h, taps_b), (taps_c_h, taps_c), (offs_h, offs),
        (tri_h, tri),
    )):
        c = pltpu.make_async_copy(src, dst, sem_v.at[j])
        c.start()
        small.append(c)
    wcopies = []
    col = 0
    for j, src in enumerate((wi, wb, wc, wk, wv, wq, wg)):
        width = src.shape[1]
        wcopies.append(pltpu.make_async_copy(src, w.at[:, pl.ds(col, width)], sem_w.at[j]))
        col += width
    for c in wcopies[:3]:
        c.start()
    n_w = len(wcopies)
    na = woa.shape[0]
    oc = [
        pltpu.make_async_copy(woa, wo.at[pl.ds(0, na)], sem_w.at[n_w]),
        pltpu.make_async_copy(wos, wo.at[pl.ds(na, wos.shape[0])], sem_w.at[n_w + 1]),
        pltpu.make_async_copy(start_hbm, start, sem_w.at[n_w + 2]),
    ]

    inner_w = wi.shape[1]
    state_w = wb.shape[1]
    xw = inner_w + 2 * state_w
    kvw = wk.shape[1]
    qw = wq.shape[1]
    gw = wg.shape[1]
    kvcol = xw
    qcol = xw + 2 * kvw
    gcol = qcol + qw
    hd2 = ws.shape[0]
    heads = hd2 // 2
    groups = state_w // STATE
    per_group = heads // groups
    gwid = per_group * HEAD
    kv_heads = kvw // HEAD
    q_per = (qw // HEAD) // kv_heads
    two = LANE // HEAD
    sq = (BLK, BLK)
    ri = lax.broadcasted_iota(jnp.int32, sq, 0)
    ci = lax.broadcasted_iota(jnp.int32, sq, 1)

    wsp[hd2:, :] = jnp.zeros((LANE - hd2, wsp.shape[1]), BF16)
    qt[...] = jnp.zeros_like(qt)
    bias_m[0] = jnp.where(ri >= ci, 0.0, NEG)
    bias_m[1] = jnp.where(ri <= ci, 0.0, NEG)
    for c in small:
        c.wait()
    wsp[0:hd2, :] = ws[...]
    qg = column(pad_row(qgain1[...] * (HEAD ** (-0.5) * LOG2E)))
    kg = column(pad_row(kgain1[...]))
    hh = HEAD // 2
    co = cos_o[idx]
    so = sin_o[idx]
    for b in range(nb):
        cols = slice(b * BLK, (b + 1) * BLK)
        c0 = cos_t[:, cols]
        s0 = sin_t[:, cols]
        cosine = co * c0 - so * s0
        sine = so * c0 + co * s0
        for k, gain in enumerate((qg, kg)):
            ga, gb = gain[0:hh], gain[hh:HEAD]
            rot[k, b, 0:hh] = ga * cosine
            rot[k, b, hh : 2 * hh] = gb * sine
            rot[k, b, 2 * hh : 3 * hh] = gb * cosine
            rot[k, b, 3 * hh : 4 * hh] = ga * sine
    bias = column(pad_row(jnp.concatenate([bias2[0:1, :], bias2[1:2, :]], axis=1)))[0:hd2]
    rate = column(pad_row(jnp.concatenate([rate2[0:1, :], rate2[1:2, :]], axis=1)))[0:hd2]
    for s in range(0, inner_w, LANE):
        ggt[s : s + LANE, :] = column(ggain[:, s : s + LANE])

    @pl.when(has_prev & has_next)
    def _():
        pl.semaphore_wait(barrier, 3)

    @pl.when(jnp.logical_not(has_prev & has_next))
    def _():
        pl.semaphore_wait(barrier, 2 if n_sp > 1 else 1)

    gath = []
    for i in range(nchunk):
        own_copies[i].wait()
        c = pltpu.make_async_remote_copy(
            src_ref=xown.at[pl.ds(i * ROWS, ROWS)],
            dst_ref=xpeer.at[pl.ds(i * ROWS, ROWS)],
            send_sem=sem_xs.at[i],
            recv_sem=sem_xr.at[i],
            device_id={"tp": peer},
            device_id_type=MESH,
        )
        c.start()
        gath.append(c)
    for c in wcopies[3:]:
        c.start()

    gain_own = mix_gain[:, pl.ds(pl.multiple_of(me * half, LANE), half)]
    gain_peer = mix_gain[:, pl.ds(pl.multiple_of(peer * half, LANE), half)]

    def scale_rows(rows, n, src, gain, base, add):
        dst = pl.multiple_of(base * half, LANE)
        total = rs[rows, :] if add else jnp.zeros((n, LANE), F32)
        for s in range(0, half, LANE):
            a = src[rows, s : s + LANE].astype(F32)
            total = total + a * a
            xs[rows, pl.ds(pl.multiple_of(dst + s, LANE), LANE)] = (
                a * gain[:, s : s + LANE]
            ).astype(BF16)
        if add:
            total = jnp.broadcast_to(
                lax.rsqrt(jnp.sum(total, axis=1, keepdims=True) * (1.0 / (2 * half)) + epsilon), (n, LANE)
            )
        rs[rows, :] = total

    def scale_own(r, carry):
        scale_rows(pl.ds(pl.multiple_of(r * 32, 32), 32), 32, xown, gain_own, me, False)
        return carry

    def scale_peer(i):
        def piece(r):
            return lambda: scale_rows(slice(r, r + 32), 32, xpeer, gain_peer, peer, True)

        return [piece(r) for r in range(i * ROWS, (i + 1) * ROWS, 32)]

    lax.fori_loop(0, T // 32, scale_own, 0, unroll=2)
    gath[0].wait()
    for piece in scale_peer(0):
        piece()

    def norm_rotate(v, k, b):
        inv = lax.rsqrt(jnp.sum(v * v, axis=0, keepdims=True) * (1.0 / HEAD) + epsilon)
        a, c = v[0:hh], v[hh:HEAD]
        first = (a * rot[k, b, 0:hh] - c * rot[k, b, hh : 2 * hh]) * inv
        second = (c * rot[k, b, 2 * hh : 3 * hh] + a * rot[k, b, 3 * hh : 4 * hh]) * inv
        return jnp.concatenate([first, second], axis=0)

    def remote(src, dst, ss, rsem, target):
        return pltpu.make_async_remote_copy(
            src_ref=src, dst_ref=dst, send_sem=ss, recv_sem=rsem,
            device_id={"sp": target}, device_id_type=MESH,
        )

    def chunk_rows(i):
        return pl.ds(pl.multiple_of(i * ROWS, ROWS), ROWS)

    def x_units(i):
        rows = chunk_rows(i)

        def step_unit():
            p = mm_t(xs[rows, :], wsp[...]) * rs[rows, :]
            pt = p.T[0:hd2]
            for u in range(per):
                b = i * per + u
                v = pt[:, u * BLK : (u + 1) * BLK] + bias
                step = jnp.maximum(v, 0.0) + jnp.log1p(jnp.exp(-jnp.abs(v)))
                st[b] = step
                ld[b] = -rate * step + offs[:, b * BLK : (b + 1) * BLK]

        def unit(s):
            def run():
                p = mm(xs[rows, :], w[:, s : s + 256])
                for t in range(0, 256, LANE):
                    xb[(s + t) // LANE, pl.ds(i * ROWS + EDGE, ROWS), :] = rounded(
                        p[:, t : t + LANE] * rs[rows, :]
                    )
            return run

        return [step_unit] + [unit(s) for s in range(0, xw, 256)]

    def kv_unit(i):
        def run():
            rows = chunk_rows(i)
            p = mm(xs[rows, :], w[:, kvcol : kvcol + 2 * kvw])
            for u in range(per):
                b = i * per + u
                part = slice(u * BLK, (u + 1) * BLK)
                scale = rs[i * ROWS + u * BLK : i * ROWS + (u + 1) * BLK, :]
                kt = rounded(p[part, :LANE] * scale).T
                kt = jnp.concatenate(
                    [norm_rotate(kt[h * HEAD : (h + 1) * HEAD], 1, b) for h in range(kv_heads)], axis=0
                )
                dst = (b + 1) * BLK
                kn[dst : dst + BLK, :] = kt.T.astype(BF16)
                vt[:, dst : dst + BLK] = (p[part, LANE:] * scale).T.astype(BF16)
        return run

    def q_units(i):
        rows = chunk_rows(i)

        def unit(s):
            def run():
                p = mm(xs[rows, :], w[:, qcol + s : qcol + s + 256])
                scale = rs[rows, :]
                for u in range(per):
                    b = i * per + u
                    part = slice(u * BLK, (u + 1) * BLK)
                    for t in range(0, 256, LANE):
                        q = rounded(p[part, t : t + LANE] * scale[part]).T
                        for v in range(two):
                            h = (s + t) // HEAD + v
                            g = h // q_per
                            qt[b, g * HEAD : (g + 1) * HEAD, h * BLK : (h + 1) * BLK] = norm_rotate(
                                q[v * HEAD : (v + 1) * HEAD], 0, b
                            ).astype(BF16)
            return run

        return [unit(s) for s in range(0, qw, 256)]

    def gate_units(i):
        rows = chunk_rows(i)

        def unit(s):
            def run():
                p = mm(xs[rows, :], w[:, gcol + s : gcol + s + 256])
                scale = rs[rows, :]
                for u in range(per):
                    part = slice(u * BLK, (u + 1) * BLK)
                    for t in range(0, 256, LANE):
                        gt[i * per + u, s + t : s + t + LANE, :] = silu(
                            rounded(p[part, t : t + LANE] * scale[part]).T
                        )
            return run

        return [unit(s) for s in range(0, gw, 256)]

    def spread(values, row, n):
        return jnp.broadcast_to(values[row : row + 1, :], (n, LANE))

    def decay_block(b):
        sums = mm(jnp.concatenate(list(pieces(ld[b])), axis=0), tri[...])
        tot = (sums[0:hd2] + sums[hd2 : 2 * hd2] + sums[2 * hd2 : 3 * hd2]) * LOG2E
        c = jnp.concatenate([tot[0:heads, 0:BLK], tot[heads:, BLK:]], axis=0)
        ct[b] = c
        end = jnp.concatenate(
            [
                jnp.broadcast_to(c[0:heads, BLK - 1 : BLK], (heads, BLK)),
                jnp.broadcast_to(c[heads:, 0:1], (heads, BLK)),
            ],
            axis=0,
        )
        dec[b] = jnp.exp2(end)
        ld[b] = st[b] * jnp.exp2(end - c)

    def state_steps(b):
        rows = slice(b * BLK, (b + 1) * BLK)

        def tile_step(tile):
            s = tile * LANE

            def run():
                if s < inner_w:
                    tap = taps_i[:, s : s + LANE].astype(F32)
                elif s < inner_w + state_w:
                    tap = taps_b[:, s - inner_w : s - inner_w + LANE].astype(F32)
                else:
                    o = s - inner_w - state_w
                    tap = taps_c[:, o : o + LANE].astype(F32)
                acc = None
                for j in range(CONV):
                    win = xb[tile, pl.ds(b * BLK + (EDGE - CONV // 2 + j), BLK), :]
                    term = win * tap[j : j + 1]
                    acc = term if acc is None else acc + term
                a = silu(acc)
                if s >= inner_w:
                    bc[rows, s - inner_w : s - inner_w + LANE] = a.astype(BF16)
                    return
                at = rounded(a.T)
                xt[b, s : s + LANE, :] = at.astype(BF16)
                g = s // gwid
                load = ld[b]
                loaded = []
                for direction in range(2):
                    for u in range(two):
                        h = tile * two + u
                        loaded.append(
                            (at[u * HEAD : (u + 1) * HEAD] * spread(load, direction * heads + h, HEAD)).astype(BF16)
                        )
                gsum = mm(jnp.concatenate(loaded, axis=0), bc[rows, g * STATE : (g + 1) * STATE])
                for direction in range(2):
                    gs[b, direction, s : s + LANE, :] = gsum[direction * LANE : (direction + 1) * LANE]
            return run

        def first():
            decay_block(b)

        order = list(range(inner_w // LANE, xw // LANE)) + list(range(inner_w // LANE))
        return [first] + [tile_step(t) for t in order]

    x_up = remote(xb.at[:, pl.ds(T, EDGE)], xhalo.at[0], sem_hs.at[2], sem_hr.at[2], idx + 1)
    x_dn = remote(xb.at[:, pl.ds(EDGE, EDGE)], xhalo.at[1], sem_hs.at[3], sem_hr.at[3], idx - 1)
    k_up = remote(kn.at[pl.ds(T, BLK)], kn.at[pl.ds(0, BLK)], sem_hs.at[0], sem_hr.at[0], idx + 1)
    k_dn = remote(kn.at[pl.ds(BLK, BLK)], kn.at[pl.ds(T + BLK, BLK)], sem_hs.at[1], sem_hr.at[1], idx - 1)
    v_up = remote(vt.at[:, pl.ds(T, BLK)], vt.at[:, pl.ds(0, BLK)], sem_hs.at[4], sem_hr.at[4], idx + 1)
    v_dn = remote(vt.at[:, pl.ds(BLK, BLK)], vt.at[:, pl.ds(T + BLK, BLK)], sem_hs.at[5], sem_hr.at[5], idx - 1)

    for c in wcopies[:3]:
        c.wait()
    for c in oc:
        c.start()

    pending = [b for b in range(1, nb - 1)]
    for i in range(nchunk):
        hosted = []
        if i + 1 < nchunk:
            gath[i + 1].wait()
            hosted += scale_peer(i + 1)
        ready = [b for b in pending if (b + 1) * BLK + CONV // 2 <= i * ROWS][:per]
        for b in ready:
            pending.remove(b)
            hosted += state_steps(b)
        with jax.named_scope("x"):
            interleave(x_units(i), hosted)
        if i == 0:
            @pl.when(has_prev)
            def _():
                x_dn.start()

    @pl.when(has_next)
    def _():
        x_up.start()

    for c in wcopies[3:]:
        c.wait()

    with jax.named_scope("kv"):
        hosted = []
        for b in pending:
            hosted += state_steps(b)
        interleave([kv_unit(i) for i in range(nchunk)], hosted)

    @pl.when(has_next)
    def _():
        k_up.start()
        v_up.start()

    @pl.when(has_prev)
    def _():
        k_dn.start()
        v_dn.start()

    @pl.when(has_next)
    def _():
        x_up.wait_send()
        x_dn.wait_recv()
        xb[:, pl.ds(T + EDGE, EDGE), :] = xhalo[1]

    @pl.when(jnp.logical_not(has_next))
    def _():
        xb[:, pl.ds(T + EDGE, EDGE), :] = jnp.zeros((xb.shape[0], EDGE, LANE), F32)

    @pl.when(has_prev)
    def _():
        x_dn.wait_send()
        x_up.wait_recv()
        xb[:, pl.ds(0, EDGE), :] = xhalo[0]

    @pl.when(jnp.logical_not(has_prev))
    def _():
        xb[:, pl.ds(0, EDGE), :] = jnp.zeros((xb.shape[0], EDGE, LANE), F32)

    with jax.named_scope("edge"):
        interleave(q_units(0), state_steps(0) + (state_steps(nb - 1) if nb > 1 else []))

    for d in range(2):
        order = list(range(nb)) if d == 0 else list(range(nb - 1, -1, -1))
        for h in range(heads):
            rows = slice(h * HEAD, (h + 1) * HEAD)
            total = gs[order[0], d, rows, :]
            for b in order[1:]:
                total = total * spread(dec[b], d * heads + h, HEAD) + gs[b, d, rows, :]
            agg[d, rows, :] = total
    prod = dec[0]
    for b in range(1, nb):
        prod = prod * dec[b]
    dtot[...] = prod

    oc[2].wait()
    hops = [
        [
            remote(
                chain_s.at[d, pl.ds(g * gwid, gwid)], chain_r.at[d, pl.ds(g * gwid, gwid)],
                sem_cs.at[d * groups + g], sem_cr.at[d * groups + g],
                idx + 1 if d == 0 else idx - 1,
            )
            for g in range(groups)
        ]
        for d in range(2)
    ]
    sources = (has_prev, has_next)
    targets = (has_next, has_prev)
    order_of = (idx, n_sp - 1 - idx)

    def hop(direction, inner):
        for g in range(groups):
            if inner:
                hops[direction][g].wait_recv()
            for u in range(per_group):
                h = g * per_group + u
                rows = slice(h * HEAD, (h + 1) * HEAD)
                enter = chain_r[direction, rows, :].astype(F32) if inner else start[direction, rows, :]
                out = enter * spread(dtot[...], direction * heads + h, HEAD) + agg[direction, rows, :]
                chain_s[direction, rows, :] = out.astype(BF16)
            hops[direction][g].start()

    for d in range(2):
        @pl.when(targets[d] & jnp.logical_not(sources[d]))
        def _(d=d):
            hop(d, False)

    slots = nchunk

    def maybe_hop(slot):
        with jax.named_scope("hop"):
            for d in range(2):
                turn = (order_of[d] * slots * 3 + 3) // (2 * n_sp)

                @pl.when((jnp.minimum(turn, slots) == slot) & targets[d] & sources[d])
                def _(d=d):
                    hop(d, True)

    @pl.when(has_next)
    def _():
        k_up.wait_send()
        v_up.wait_send()
        k_dn.wait_recv()
        v_dn.wait_recv()

    @pl.when(jnp.logical_not(has_next))
    def _():
        kn[pl.ds(T + BLK, BLK), :] = jnp.zeros((BLK, kvw), BF16)
        vt[:, pl.ds(T + BLK, BLK)] = jnp.zeros((kvw, BLK), BF16)

    @pl.when(has_prev)
    def _():
        k_dn.wait_send()
        v_dn.wait_send()
        k_up.wait_recv()
        v_up.wait_recv()

    @pl.when(jnp.logical_not(has_prev))
    def _():
        kn[pl.ds(0, BLK), :] = jnp.zeros((BLK, kvw), BF16)
        vt[:, pl.ds(0, BLK)] = jnp.zeros((kvw, BLK), BF16)

    key_w = 3 * BLK
    ones = jnp.ones((16, key_w), BF16)
    sinks = sink[...] * LOG2E
    pairs = qw // HEAD // 2

    def attend_chunk(i, hosted):
        todo = [(i * per + u, p) for u in range(per) for p in range(pairs)]
        los = {}

        def scores(n):
            b, p = todo[n]
            return mm(kn[b * BLK : b * BLK + key_w, :], qt[b, :, 2 * p * BLK : 2 * (p + 1) * BLK])

        def weigh(n, s_all):
            b, p = todo[n]
            lo, hi = bias_m[0], bias_m[1]
            if b == 0:
                lo = lo + jnp.where(idx == 0, NEG, 0.0)
            if b == nb - 1:
                hi = hi + jnp.where(idx == n_sp - 1, NEG, 0.0)
            probs, adds = [], []
            for u in range(2):
                h = 2 * p + u
                s = s_all[:, u * BLK : (u + 1) * BLK]
                s = jnp.concatenate([s[0:BLK] + lo, s[BLK : 2 * BLK], s[2 * BLK :] + hi], axis=0)
                sk = jnp.broadcast_to(sinks[:, h : h + 1], (1, BLK))
                m = jnp.maximum(jnp.max(s, axis=0, keepdims=True), sk)
                probs.append(jnp.exp2(s - m).astype(BF16))
                adds.append(jnp.exp2(sk - m))
            return jnp.concatenate(probs, axis=1), adds

        def value(n, probs, adds):
            b, p = todo[n]
            g = 2 * p // q_per
            vals = jnp.concatenate([vt[g * HEAD : (g + 1) * HEAD, b * BLK : b * BLK + key_w], ones], axis=0)
            o = mm(vals, probs)
            outs = []
            for u in range(2):
                cols = slice(u * BLK, (u + 1) * BLK)
                inv = 1.0 / (o[HEAD : HEAD + 1, cols] + adds[u])
                outs.append(o[0:HEAD, cols] * inv)
            z[b * BLK : (b + 1) * BLK, p * LANE : (p + 1) * LANE] = (
                jnp.concatenate(outs, axis=0).T.astype(BF16)
            )

        state = {0: scores(0)}

        def step(n):
            def run():
                if n + 1 < len(todo):
                    state[n + 1] = scores(n + 1)
                state[n] = weigh(n, state[n])
            return run

        def close(n):
            return lambda: value(n, *state.pop(n))

        done = 0
        for n in range(len(todo)):
            step(n)()
            want = ((n + 1) * len(hosted)) // len(todo)
            while done < want:
                hosted[done]()
                done += 1
            close(n)()

    for i in range(nchunk):
        maybe_hop(i)
        with jax.named_scope("attend"):
            attend_chunk(i, (q_units(i + 1) if i + 1 < nchunk else []) + gate_units(i))
    maybe_hop(nchunk)

    with jax.named_scope("w_chain"):
        for d in range(2):
            @pl.when(targets[d])
            def _(d=d):
                for c in hops[d]:
                    c.wait_send()

            @pl.when(sources[d] & jnp.logical_not(targets[d]))
            def _(d=d):
                for c in hops[d]:
                    c.wait_recv()

    for d in range(2):
        order = list(range(nb)) if d == 0 else list(range(nb - 1, -1, -1))
        for h in range(heads):
            rows = slice(h * HEAD, (h + 1) * HEAD)
            total = jnp.where(sources[d], chain_r[d, rows, :].astype(F32), start[d, rows, :])
            for b in order:
                sb[b, d, rows, :] = total.astype(BF16)
                if b != order[-1]:
                    total = total * spread(dec[b], d * heads + h, HEAD) + gs[b, d, rows, :]

    attn_w = qw
    zero_pad = jnp.zeros((LANE - hd2, LANE), F32)

    def mix_steps(b):
        rows = pl.ds(pl.multiple_of(b * BLK, BLK), BLK)
        env = {}

        def begin():
            c = ct[b]
            step = st[b]
            e = c - jnp.log2(jnp.maximum(step, 1e-37))
            env["c"] = c
            env["en"] = jnp.concatenate([e, zero_pad], axis=0).T
            env["both"] = jnp.log2(jnp.maximum(step[0:heads] + step[heads:], 1e-37))
            env["grow"] = jnp.exp2(c)

        def open_group(g):
            def run():
                bm = bc[rows, g * STATE : (g + 1) * STATE]
                cm = bc[rows, state_w + g * STATE : state_w + (g + 1) * STATE]
                env["scores"] = mm_t(bm, cm)
                states = jnp.concatenate(
                    [sb[b, d, g * gwid : (g + 1) * gwid, :] for d in range(2)], axis=0
                )
                env["carried"] = mm_t(states, cm)
                env["gated"] = []
            return run

        def head(g, u):
            def run():
                h = g * per_group + u
                c, en, carried, grow = env["c"], env["en"], env["carried"], env["grow"]
                arg = jnp.where(
                    ri < ci,
                    spread(c, h, BLK) - jnp.broadcast_to(en[:, h : h + 1], sq),
                    spread(c, heads + h, BLK) - jnp.broadcast_to(en[:, heads + h : heads + h + 1], sq),
                )
                arg = jnp.where(ri == ci, spread(env["both"], h, BLK), arg)
                weights = (env["scores"] * jnp.exp2(arg)).astype(BF16)
                y = mm(xt[b, h * HEAD : (h + 1) * HEAD, :], weights)
                y = y + carried[u * HEAD : (u + 1) * HEAD] * spread(grow, h, HEAD)
                y = y + carried[gwid + u * HEAD : gwid + (u + 1) * HEAD] * spread(grow, heads + h, HEAD)
                env["gated"].append(y * gt[b, h * HEAD : (h + 1) * HEAD, :])
            return run

        def close_group(g):
            def run():
                gated = env["gated"]
                total = sum(jnp.sum(v * v, axis=0, keepdims=True) for v in gated)
                inv = lax.rsqrt(total * (1.0 / gwid) + epsilon)
                for t in range(per_group // 2):
                    s = g * gwid + t * LANE
                    v = jnp.concatenate([gated[2 * t], gated[2 * t + 1]], axis=0)
                    z[rows, attn_w + s : attn_w + s + LANE] = (v * inv * ggt[s : s + LANE, :]).T.astype(BF16)
            return run

        steps = [begin]
        for g in range(groups):
            steps.append(open_group(g))
            steps += [head(g, u) for u in range(per_group)]
            steps.append(close_group(g))
        return steps

    for c in oc[:2]:
        c.wait()
    half_rows = T // 2
    steps = half_rows // ROWS
    width = wo.shape[1]
    copies = [
        pltpu.make_async_remote_copy(
            src_ref=psend.at[pl.ds(i * ROWS, ROWS)],
            dst_ref=precv.at[pl.ds(i * ROWS, ROWS)],
            send_sem=sem_ps.at[i],
            recv_sem=sem_pr.at[i],
            device_id={"tp": peer},
            device_id_type=MESH,
        )
        for i in range(steps)
    ]

    def chunk_base(k):
        owner = peer if k < steps else me
        return owner * half_rows + (k % steps) * ROWS

    def out_units(k):
        zr = pl.ds(pl.multiple_of(chunk_base(k), ROWS), ROWS)
        i = k % steps
        dst = slice(i * ROWS, (i + 1) * ROWS)

        def unit(s):
            def run():
                part = mm(z[zr, :], wo[:, s : s + 256])
                if k < steps:
                    psend[dst, s : s + 256] = part.astype(BF16)
                else:
                    outv[dst, s : s + 256] = (
                        rounded(part) + precv[dst, s : s + 256].astype(F32)
                    ).astype(BF16)
            return run

        return [unit(s) for s in range(0, width, 256)]

    total_chunks = 2 * steps
    for k in range(total_chunks + 1):
        if k > steps:
            with jax.named_scope("w_p"):
                copies[k - 1 - steps].wait()
        with jax.named_scope("mix"):
            hosted = out_units(k - 1) if k > 0 else []
            main = []
            if k < total_chunks:
                for u in range(per):
                    main += mix_steps(chunk_base(k) // BLK + u)
            if main:
                interleave(main, hosted)
            else:
                for piece in hosted:
                    piece()
        if 0 < k <= steps:
            copies[k - 1].start()


def tables(tokens, count):
    half = HEAD // 2
    frequency = rotary_base ** (-np.arange(half, dtype=np.float64) / half)
    inner = frequency[:, None] * np.arange(tokens, dtype=np.float64)[None, :]
    outer = np.arange(count, dtype=np.float64)[:, None] * tokens * frequency[None, :]
    outer = np.broadcast_to(outer[:, :, None], (count, half, LANE))
    return [f(a).astype(np.float32) for a in (inner, outer) for f in (np.cos, np.sin)]


def local(
    n_sp,
    inputs, mix_gain, w_query, w_key, w_value, query_gain, key_gain, sink_logit,
    w_inner, w_bmat, w_cmat, w_gate, w_step, conv_inner, conv_bmat, conv_cmat,
    step_bias, decay_rate, decay_offset, start_state, group_gain, w_out_attn, w_out_state,
):
    T, half = inputs.shape
    depth = w_query.shape[0]
    heads = w_step.shape[2]
    inner_w = w_inner.shape[1]
    state_w = w_bmat.shape[1]
    xw = inner_w + 2 * state_w
    kvw = w_key.shape[1]
    qw = w_query.shape[1]
    gw = w_gate.shape[1]
    width = w_out_attn.shape[1]
    nb = T // BLK
    nchunk = T // ROWS
    groups = state_w // STATE

    ws = jnp.transpose(w_step, (1, 2, 0)).reshape(2 * heads, depth)
    offs = jnp.transpose(decay_offset, (1, 2, 0)).reshape(2 * heads, T)
    start = start_state.reshape(2, inner_w, STATE)
    ct, sn, co, so = tables(T, n_sp)
    tri = np.triu(np.ones((BLK, BLK), np.float32))
    tri = np.concatenate([tri, tri.T], axis=1)
    any_spec = pl.BlockSpec(memory_space=pl.ANY)
    vm = pl.BlockSpec(memory_space=pltpu.VMEM)
    wcols = 2 * kvw + xw + qw + gw
    V = pltpu.VMEM
    dma = pltpu.SemaphoreType.DMA
    steps = T // 2 // ROWS
    hd2 = 2 * heads
    small = [
        ws, mix_gain.reshape(1, -1), query_gain.reshape(1, -1), key_gain.reshape(1, -1),
        sink_logit.reshape(1, -1), conv_inner, conv_bmat, conv_cmat, step_bias, decay_rate,
        offs, group_gain.reshape(1, -1), jnp.asarray(ct), jnp.asarray(sn), jnp.asarray(co),
        jnp.asarray(so), jnp.asarray(tri, dtype=BF16),
    ]
    scratch = [V(a.shape, a.dtype) for a in small] + [
        V((depth, wcols), BF16), V((LANE, depth), BF16),
        V((w_out_attn.shape[0] + w_out_state.shape[0], width), BF16),
        V((2, inner_w, STATE), F32),
        V((T, half), BF16), V((T, half), BF16), V((T, 2 * half), BF16), V((T, LANE), F32),
        V((2, nb, 2 * HEAD, LANE), F32),
        V((T + 2 * BLK, kvw), BF16), V((kvw, T + 2 * BLK), BF16),
        V((xw // LANE, T + 2 * EDGE, LANE), F32),
        V((nb, kvw, qw // HEAD * BLK), BF16), V((nb, gw, BLK), F32),
        V((T, 2 * state_w), BF16), V((nb, inner_w, BLK), BF16),
        V((nb, hd2, BLK), F32), V((nb, hd2, BLK), F32), V((nb, hd2, BLK), F32), V((nb, hd2, BLK), F32),
        V((inner_w, LANE), F32), V((2, BLK, BLK), F32),
        V((nb, 2, inner_w, STATE), F32), V((2, inner_w, STATE), F32), V((hd2, LANE), F32),
        V((nb, 2, inner_w, STATE), BF16),
        V((T, qw + inner_w), BF16),
        V((T // 2, width), BF16), V((T // 2, width), BF16),
        V((2, xw // LANE, EDGE, LANE), F32),
        V((2, inner_w, STATE), BF16), V((2, inner_w, STATE), BF16),
        dma((len(small),)), dma((10,)), dma((nchunk,)), dma((nchunk,)), dma((nchunk,)),
        dma((6,)), dma((6,)), dma((2 * groups,)), dma((2 * groups,)), dma((steps,)), dma((steps,)),
    ]
    return pl.pallas_call(
        functools.partial(kernel, n_sp=n_sp),
        out_shape=pltpu.VMEM((T // 2, width), BF16),
        in_specs=[any_spec] * (11 + len(small)),
        out_specs=vm,
        scratch_shapes=scratch,
        compiler_params=pltpu.CompilerParams(
            collective_id=0, has_side_effects=True, vmem_limit_bytes=58720256
        ),
        name="mixer",
    )(
        inputs, w_query, w_key, w_value, w_inner, w_bmat, w_cmat, w_gate,
        w_out_attn, w_out_state, start, *small,
    )


def solution(mesh):
    return jax.shard_map(
        functools.partial(local, mesh.shape["sp"]),
        mesh=mesh,
        in_specs=(
            P(("fs", "sp"), "tp"),
            P(),
            P(None, "tp"),
            P(None, "tp"),
            P(None, "tp"),
            P(),
            P(),
            P("tp"),
            P(None, "tp"),
            P(None, "tp"),
            P(None, "tp"),
            P(None, "tp"),
            P(None, None, "tp"),
            P(None, "tp"),
            P(None, "tp"),
            P(None, "tp"),
            P(None, "tp"),
            P(None, "tp"),
            P("sp", None, "tp"),
            P("fs", "tp", None, None),
            P("tp"),
            P("tp", None),
            P("tp", None),
        ),
        out_specs=P(("fs", "sp", "tp"), None),
        check_vma=False,
    )
```

```python
import functools

import jax
import jax.numpy as jnp
import numpy as np
from jax import lax
from jax.experimental import pallas as pl
from jax.experimental.pallas import tpu as pltpu
from jax.sharding import PartitionSpec as P

HEAD = 64
STATE = 128
CONV = 5
BLK = 128
LANE = 128
ROWS = 256
EDGE = 8

epsilon = 1e-06
rotary_base = 10000.0
LOG2E = 1.4426950408889634
NEG = -1e30
F32 = jnp.float32
BF16 = jnp.bfloat16
MESH = pl.DeviceIdType.MESH


def mm(a, b):
    return jnp.dot(a, b, preferred_element_type=F32)


def mm_t(a, b):
    return lax.dot_general(a, b, (((1,), (1,)), ((), ())), preferred_element_type=F32)


def silu_of_twice(v):
    return v + v * jnp.tanh(v)


def rounded(v):
    return v.astype(BF16).astype(F32)


def column(row):
    return jnp.broadcast_to(row, (LANE, LANE)).T


def pad_row(row):
    return jnp.concatenate([row, jnp.zeros((1, LANE - row.shape[1]), F32)], axis=1)


def pieces(v):
    hi = v.astype(BF16)
    rest = v - hi.astype(F32)
    mid = rest.astype(BF16)
    lo = (rest - mid.astype(F32)).astype(BF16)
    return hi, mid, lo


def pipeline(items):
    active = []
    for item in items:
        stages = item()
        if stages is None:
            continue
        active = [g for g in active + [stages] if next(g, True) is None]
    while active:
        active = [g for g in active if next(g, True) is None]


def blend(main, extra):
    out, done = [], 0
    for i, item in enumerate(main):
        out.append(item)
        want = ((i + 1) * len(extra)) // len(main)
        out += extra[done:want]
        done = want
    return out + extra[done:]


def kernel(
    x_hbm, wq, wk, wv, wi, wb, wc, wg, woa, wos, start_hbm,
    ws_h, mix_gain_h, qgain_h, kgain_h, sink_h, taps_i_h, taps_b_h, taps_c_h, bias_h, rate_h, offs_h,
    ggain_h, cos_t_h, sin_t_h, cos_o_h, sin_o_h, tri_h,
    outv,
    ws, mix_gain, qgain1, kgain1, sink, taps_i, taps_b, taps_c, bias2, rate2, offs,
    ggain, cos_t, sin_t, cos_o, sin_o, tri,
    w, wsp, wo, start, xown, xpeer, xa, xp, rs, rot, kn, vt, xb, qt, gt, bc, xt, st, ct, dec, ld, ggt, bias_m,
    gs, agg, dtot, sb, ys, z, zs0, zs1, zs2, zs3, psend, precv, xhalo, chain_s, chain_r,
    sem_v, sem_w, sem_x, sem_xs, sem_xr, sem_hs, sem_hr, sem_cs, sem_cr, sem_ps, sem_pr,
    *, n_sp,
):
    zs = (zs0, zs1, zs2, zs3)
    me = lax.axis_index("tp")
    idx = lax.axis_index("sp")
    peer = 1 - me
    T, half = x_hbm.shape
    nb = T // BLK
    nchunk = T // ROWS
    per = ROWS // BLK
    has_prev = idx > 0
    has_next = idx < n_sp - 1

    first = [0] + ([nchunk - 1] if nchunk > 1 else [])
    trail = first + [i for i in range(nchunk) if i not in first]
    own_copies = {}
    for i in trail:
        c = pltpu.make_async_copy(
            x_hbm.at[pl.ds(i * ROWS, ROWS)], xown.at[pl.ds(i * ROWS, ROWS)], sem_x.at[i]
        )
        c.start()
        own_copies[i] = c

    barrier = pltpu.get_barrier_semaphore()
    pl.semaphore_signal(barrier, inc=1, device_id={"tp": peer}, device_id_type=MESH)

    @pl.when(has_prev)
    def _():
        pl.semaphore_signal(barrier, inc=1, device_id={"sp": idx - 1}, device_id_type=MESH)

    @pl.when(has_next)
    def _():
        pl.semaphore_signal(barrier, inc=1, device_id={"sp": idx + 1}, device_id_type=MESH)

    small = []
    for j, (src, dst) in enumerate((
        (mix_gain_h, mix_gain), (qgain_h, qgain1), (kgain_h, kgain1), (cos_o_h, cos_o), (sin_o_h, sin_o),
        (cos_t_h, cos_t), (sin_t_h, sin_t), (bias_h, bias2), (rate_h, rate2), (ggain_h, ggain), (ws_h, ws),
        (sink_h, sink), (taps_i_h, taps_i), (taps_b_h, taps_b), (taps_c_h, taps_c), (offs_h, offs),
        (tri_h, tri),
    )):
        c = pltpu.make_async_copy(src, dst, sem_v.at[j])
        c.start()
        small.append(c)
    wcopies = []
    col = 0
    own_rows = pl.ds(pl.multiple_of(me * half, LANE), half)
    peer_rows = pl.ds(pl.multiple_of(peer * half, LANE), half)
    for j, src in enumerate((wi, wb, wc, wk, wv, wq, wg)):
        width = src.shape[1]
        for k, part in enumerate((own_rows, peer_rows)):
            wcopies.append(
                pltpu.make_async_copy(
                    src.at[part], w.at[pl.ds(k * half, half), pl.ds(col, width)], sem_w.at[2 * j + k]
                )
            )
        col += width
    for c in wcopies[:6]:
        c.start()
    n_w = len(wcopies)
    na = woa.shape[0]
    oc = [
        pltpu.make_async_copy(woa, wo.at[pl.ds(0, na)], sem_w.at[n_w]),
        pltpu.make_async_copy(wos, wo.at[pl.ds(na, wos.shape[0])], sem_w.at[n_w + 1]),
        pltpu.make_async_copy(start_hbm, start, sem_w.at[n_w + 2]),
    ]

    inner_w = wi.shape[1]
    state_w = wb.shape[1]
    xw = inner_w + 2 * state_w
    kvw = wk.shape[1]
    qw = wq.shape[1]
    gw = wg.shape[1]
    kvcol = xw
    qcol = xw + 2 * kvw
    gcol = qcol + qw
    hd2 = ws.shape[0]
    heads = hd2 // 2
    groups = state_w // STATE
    per_group = heads // groups
    gwid = per_group * HEAD
    kv_heads = kvw // HEAD
    q_per = (qw // HEAD) // kv_heads
    two = LANE // HEAD
    sq = (BLK, BLK)
    ri = lax.broadcasted_iota(jnp.int32, sq, 0)
    ci = lax.broadcasted_iota(jnp.int32, sq, 1)

    wsp[hd2:, :] = jnp.zeros((LANE - hd2, wsp.shape[1]), BF16)
    qt[...] = jnp.zeros_like(qt)
    bias_m[0] = jnp.where(ri >= ci, 0.0, NEG)
    bias_m[1] = jnp.where(ri <= ci, 0.0, NEG)
    for c in small:
        c.wait()
    wsp[0:hd2, 0:half] = ws[:, own_rows]
    wsp[0:hd2, half:] = ws[:, peer_rows]
    qg = column(pad_row(qgain1[...] * (HEAD ** (-0.5) * LOG2E)))
    kg = column(pad_row(kgain1[...]))
    hh = HEAD // 2
    co = cos_o[idx]
    so = sin_o[idx]
    for b in range(nb):
        cols = slice(b * BLK, (b + 1) * BLK)
        c0 = cos_t[:, cols]
        s0 = sin_t[:, cols]
        cosine = co * c0 - so * s0
        sine = so * c0 + co * s0
        for k, gain in enumerate((qg, kg)):
            ga, gb = gain[0:hh], gain[hh:HEAD]
            rot[k, b, 0:hh] = ga * cosine
            rot[k, b, hh : 2 * hh] = gb * sine
            rot[k, b, 2 * hh : 3 * hh] = gb * cosine
            rot[k, b, 3 * hh : 4 * hh] = ga * sine
    bias = column(pad_row(jnp.concatenate([bias2[0:1, :], bias2[1:2, :]], axis=1)))[0:hd2]
    rate = column(pad_row(jnp.concatenate([rate2[0:1, :], rate2[1:2, :]], axis=1)))[0:hd2]
    for s in range(0, inner_w, LANE):
        ggt[s : s + LANE, :] = column(ggain[:, s : s + LANE])

    @pl.when(has_prev & has_next)
    def _():
        pl.semaphore_wait(barrier, 3)

    @pl.when(jnp.logical_not(has_prev & has_next))
    def _():
        pl.semaphore_wait(barrier, 2 if n_sp > 1 else 1)

    gath = {}
    for i in trail:
        own_copies[i].wait()
        c = pltpu.make_async_remote_copy(
            src_ref=xown.at[pl.ds(i * ROWS, ROWS)],
            dst_ref=xpeer.at[pl.ds(i * ROWS, ROWS)],
            send_sem=sem_xs.at[i],
            recv_sem=sem_xr.at[i],
            device_id={"tp": peer},
            device_id_type=MESH,
        )
        c.start()
        gath[i] = c
    for c in wcopies[6:]:
        c.start()

    gain_own = mix_gain[:, pl.ds(pl.multiple_of(me * half, LANE), half)]
    gain_peer = mix_gain[:, pl.ds(pl.multiple_of(peer * half, LANE), half)]

    def scale_rows(rows, n, src, gain, dst, add):
        total = rs[rows, :] if add else jnp.zeros((n, LANE), F32)
        for s in range(0, half, LANE):
            a = src[rows, s : s + LANE].astype(F32)
            total = total + a * a
            dst[rows, s : s + LANE] = (a * gain[:, s : s + LANE]).astype(BF16)
        if add:
            total = jnp.broadcast_to(
                lax.rsqrt(jnp.sum(total, axis=1, keepdims=True) * (1.0 / (2 * half)) + epsilon), (n, LANE)
            )
        rs[rows, :] = total

    def scale_own(r, carry):
        scale_rows(pl.ds(pl.multiple_of(r * 32, 32), 32), 32, xown, gain_own, xa, False)
        return carry

    def scale_peer(i):
        def piece(r):
            def run():
                scale_rows(slice(r, r + 32), 32, xpeer, gain_peer, xp, True)
            return run

        return [piece(r) for r in range(i * ROWS, (i + 1) * ROWS, 32)]

    lax.fori_loop(0, T // 32, scale_own, 0, unroll=2)
    gath[0].wait()
    for piece in scale_peer(0):
        piece()

    def norm_rotate(v, k, b):
        inv = lax.rsqrt(jnp.sum(v * v, axis=0, keepdims=True) * (1.0 / HEAD) + epsilon)
        a, c = v[0:hh], v[hh:HEAD]
        first = (a * rot[k, b, 0:hh] - c * rot[k, b, hh : 2 * hh]) * inv
        second = (c * rot[k, b, 2 * hh : 3 * hh] + a * rot[k, b, 3 * hh : 4 * hh]) * inv
        return jnp.concatenate([first, second], axis=0)

    def remote(src, dst, ss, rsem, target):
        return pltpu.make_async_remote_copy(
            src_ref=src, dst_ref=dst, send_sem=ss, recv_sem=rsem,
            device_id={"sp": target}, device_id_type=MESH,
        )

    def chunk_rows(i):
        return slice(i * ROWS, (i + 1) * ROWS)

    def project(rows, lo, hi):
        return mm(xa[rows, :], w[0:half, lo:hi]) + mm(xp[rows, :], w[half:, lo:hi])

    def x_units(i):
        rows = chunk_rows(i)

        def step_unit():
            p = mm_t(xa[rows, :], wsp[:, 0:half]) + mm_t(xp[rows, :], wsp[:, half:])
            yield
            pt = (p * rs[rows, :]).T[0:hd2]
            for u in range(per):
                b = i * per + u
                v = pt[:, u * BLK : (u + 1) * BLK] + bias
                step = jnp.maximum(v, 0.0) + jnp.log1p(jnp.exp(-jnp.abs(v)))
                st[b] = step
                ld[b] = -rate * step + offs[:, b * BLK : (b + 1) * BLK]

        def unit(s):
            def run():
                p = project(rows, s, s + 256)
                yield
                for t in range(0, 256, LANE):
                    xb[(s + t) // LANE, pl.ds(i * ROWS + EDGE, ROWS), :] = rounded(
                        p[:, t : t + LANE] * rs[rows, :]
                    )
            return run

        return [step_unit] + [unit(s) for s in range(0, xw, 256)]

    def kv_unit(i):
        def run():
            rows = chunk_rows(i)
            p = project(rows, kvcol, kvcol + 2 * kvw)
            yield
            for u in range(per):
                b = i * per + u
                part = slice(u * BLK, (u + 1) * BLK)
                scale = rs[i * ROWS + u * BLK : i * ROWS + (u + 1) * BLK, :]
                kt = rounded(p[part, :LANE] * scale).T
                kt = jnp.concatenate(
                    [norm_rotate(kt[h * HEAD : (h + 1) * HEAD], 1, b) for h in range(kv_heads)], axis=0
                )
                dst = (b + 1) * BLK
                kn[dst : dst + BLK, :] = kt.T.astype(BF16)
                vt[:, dst : dst + BLK] = (p[part, LANE:] * scale).T.astype(BF16)
        return run

    def q_units(i):
        rows = chunk_rows(i)

        def unit(s):
            def run():
                p = project(rows, qcol + s, qcol + s + 256)
                yield
                scale = rs[rows, :]
                for u in range(per):
                    b = i * per + u
                    part = slice(u * BLK, (u + 1) * BLK)
                    for t in range(0, 256, LANE):
                        q = rounded(p[part, t : t + LANE] * scale[part]).T
                        for v in range(two):
                            h = (s + t) // HEAD + v
                            g = h // q_per
                            qt[b, g * HEAD : (g + 1) * HEAD, h * BLK : (h + 1) * BLK] = norm_rotate(
                                q[v * HEAD : (v + 1) * HEAD], 0, b
                            ).astype(BF16)
            return run

        return [unit(s) for s in range(0, qw, 256)]

    def gate_units(i):
        rows = chunk_rows(i)

        def unit(s):
            def run():
                p = project(rows, gcol + s, gcol + s + 256)
                yield
                scale = rs[rows, :]
                for u in range(per):
                    part = slice(u * BLK, (u + 1) * BLK)
                    for t in range(0, 256, LANE):
                        gt[i * per + u, s + t : s + t + LANE, :] = silu_of_twice(
                            0.5 * rounded(p[part, t : t + LANE] * scale[part]).T
                        )
            return run

        return [unit(s) for s in range(0, gw, 256)]

    def spread(values, row, n):
        return jnp.broadcast_to(values[row : row + 1, :], (n, LANE))

    def decay_block(b):
        sums = mm(jnp.concatenate(list(pieces(ld[b])), axis=0), tri[...])
        yield
        tot = (sums[0:hd2] + sums[hd2 : 2 * hd2] + sums[2 * hd2 : 3 * hd2]) * LOG2E
        c = jnp.concatenate([tot[0:heads, 0:BLK], tot[heads:, BLK:]], axis=0)
        ct[b] = c
        end = jnp.concatenate(
            [
                jnp.broadcast_to(c[0:heads, BLK - 1 : BLK], (heads, BLK)),
                jnp.broadcast_to(c[heads:, 0:1], (heads, BLK)),
            ],
            axis=0,
        )
        dec[b] = jnp.exp2(end)
        ld[b] = st[b] * jnp.exp2(end - c)

    def state_steps(b):
        rows = slice(b * BLK, (b + 1) * BLK)

        def tile_step(tile):
            s = tile * LANE

            def run():
                if s < inner_w:
                    tap = 0.5 * taps_i[:, s : s + LANE].astype(F32)
                elif s < inner_w + state_w:
                    tap = 0.5 * taps_b[:, s - inner_w : s - inner_w + LANE].astype(F32)
                else:
                    o = s - inner_w - state_w
                    tap = 0.5 * taps_c[:, o : o + LANE].astype(F32)
                acc = None
                for j in range(CONV):
                    win = xb[tile, pl.ds(b * BLK + (EDGE - CONV // 2 + j), BLK), :]
                    term = win * tap[j : j + 1]
                    acc = term if acc is None else acc + term
                a = silu_of_twice(acc)
                if s >= inner_w:
                    bc[rows, s - inner_w : s - inner_w + LANE] = a.astype(BF16)
                    return
                at = rounded(a.T)
                xt[b, s : s + LANE, :] = at.astype(BF16)
                g = s // gwid
                load = ld[b]
                loaded = []
                for direction in range(2):
                    for u in range(two):
                        h = tile * two + u
                        loaded.append(
                            (at[u * HEAD : (u + 1) * HEAD] * spread(load, direction * heads + h, HEAD)).astype(BF16)
                        )
                yield
                gsum = mm(jnp.concatenate(loaded, axis=0), bc[rows, g * STATE : (g + 1) * STATE])
                yield
                for direction in range(2):
                    gs[b, direction, s : s + LANE, :] = gsum[direction * LANE : (direction + 1) * LANE]
            return run

        def first():
            return decay_block(b)

        order = list(range(inner_w // LANE, xw // LANE)) + list(range(inner_w // LANE))
        return [first] + [tile_step(t) for t in order]

    x_up = remote(xb.at[:, pl.ds(T, EDGE)], xhalo.at[0], sem_hs.at[2], sem_hr.at[2], idx + 1)
    x_dn = remote(xb.at[:, pl.ds(EDGE, EDGE)], xhalo.at[1], sem_hs.at[3], sem_hr.at[3], idx - 1)
    k_up = remote(kn.at[pl.ds(T, BLK)], kn.at[pl.ds(0, BLK)], sem_hs.at[0], sem_hr.at[0], idx + 1)
    k_dn = remote(kn.at[pl.ds(BLK, BLK)], kn.at[pl.ds(T + BLK, BLK)], sem_hs.at[1], sem_hr.at[1], idx - 1)
    v_up = remote(vt.at[:, pl.ds(T, BLK)], vt.at[:, pl.ds(0, BLK)], sem_hs.at[4], sem_hr.at[4], idx + 1)
    v_dn = remote(vt.at[:, pl.ds(BLK, BLK)], vt.at[:, pl.ds(T + BLK, BLK)], sem_hs.at[5], sem_hr.at[5], idx - 1)

    for c in wcopies[:6]:
        c.wait()
    for c in oc:
        c.start()

    def action(f):
        def run():
            f()
        return run

    visit = list(range(1, nchunk - 1)) + [0] + ([nchunk - 1] if nchunk > 1 else [])
    pending = [b for b in range(1, nb - 1)]

    def send_rims():
        @pl.when(has_prev)
        def _():
            x_dn.start()

        @pl.when(has_next)
        def _():
            x_up.start()

    def wait_rims():
        @pl.when(has_next)
        def _():
            x_up.wait_send()
            x_dn.wait_recv()
            xb[:, pl.ds(T + EDGE, EDGE), :] = xhalo[1]

        @pl.when(jnp.logical_not(has_next))
        def _():
            xb[:, pl.ds(T + EDGE, EDGE), :] = jnp.zeros((xb.shape[0], EDGE, LANE), F32)

        @pl.when(has_prev)
        def _():
            x_dn.wait_send()
            x_up.wait_recv()
            xb[:, pl.ds(0, EDGE), :] = xhalo[0]

        @pl.when(jnp.logical_not(has_prev))
        def _():
            xb[:, pl.ds(0, EDGE), :] = jnp.zeros((xb.shape[0], EDGE, LANE), F32)

    seq = []
    done = []
    for n, i in enumerate(trail):
        hosted = []
        if n + 1 < nchunk:
            seq.append(action(gath[trail[n + 1]].wait))
            hosted += scale_peer(trail[n + 1])
        ready = [
            b for b in pending
            if (b * BLK - CONV // 2) // ROWS in done and ((b + 1) * BLK + CONV // 2 - 1) // ROWS in done
        ][:per]
        for b in ready:
            pending.remove(b)
            hosted += state_steps(b)
        units = blend(x_units(i), hosted)
        if n == len(first):
            units.insert(2, action(send_rims))
        seq += units
        done.append(i)
    with jax.named_scope("x"):
        pipeline(seq)
    if nchunk <= len(first):
        send_rims()

    for c in wcopies[6:]:
        c.wait()

    def send_kv():
        @pl.when(has_next)
        def _():
            k_up.start()
            v_up.start()

        @pl.when(has_prev)
        def _():
            k_dn.start()
            v_dn.start()

    inner_steps = []
    for b in pending:
        inner_steps += state_steps(b)
    seq = blend(inner_steps, [kv_unit(i) for i in range(nchunk)])
    rims = blend(
        state_steps(0) + (state_steps(nb - 1) if nb > 1 else []), q_units(visit[0])
    )
    rims.insert(2, action(send_kv))
    with jax.named_scope("kv"):
        pipeline(seq + [action(wait_rims)] + rims)

    for d in range(2):
        order = list(range(nb)) if d == 0 else list(range(nb - 1, -1, -1))
        for h in range(heads):
            rows = slice(h * HEAD, (h + 1) * HEAD)
            total = gs[order[0], d, rows, :]
            for b in order[1:]:
                total = total * spread(dec[b], d * heads + h, HEAD) + gs[b, d, rows, :]
            agg[d, rows, :] = total
    prod = dec[0]
    for b in range(1, nb):
        prod = prod * dec[b]
    dtot[...] = prod

    oc[2].wait()
    hops = [
        [
            remote(
                chain_s.at[d, pl.ds(g * gwid, gwid)], chain_r.at[d, pl.ds(g * gwid, gwid)],
                sem_cs.at[d * groups + g], sem_cr.at[d * groups + g],
                idx + 1 if d == 0 else idx - 1,
            )
            for g in range(groups)
        ]
        for d in range(2)
    ]
    sources = (has_prev, has_next)
    targets = (has_next, has_prev)
    order_of = (idx, n_sp - 1 - idx)

    def hop(direction, inner):
        for g in range(groups):
            if inner:
                hops[direction][g].wait_recv()
            for u in range(per_group):
                h = g * per_group + u
                rows = slice(h * HEAD, (h + 1) * HEAD)
                enter = chain_r[direction, rows, :].astype(F32) if inner else start[direction, rows, :]
                out = enter * spread(dtot[...], direction * heads + h, HEAD) + agg[direction, rows, :]
                chain_s[direction, rows, :] = out.astype(BF16)
            hops[direction][g].start()

    for d in range(2):
        @pl.when(targets[d] & jnp.logical_not(sources[d]))
        def _(d=d):
            hop(d, False)

    slots = nchunk

    def maybe_hop(slot):
        with jax.named_scope("hop"):
            for d in range(2):
                turn = jnp.maximum((order_of[d] * slots * 2) // n_sp, 1)

                @pl.when((jnp.minimum(turn, slots) == slot) & targets[d] & sources[d])
                def _(d=d):
                    hop(d, True)

    def kv_halo():
        @pl.when(has_next)
        def _():
            k_up.wait_send()
            v_up.wait_send()
            k_dn.wait_recv()
            v_dn.wait_recv()

        @pl.when(jnp.logical_not(has_next))
        def _():
            kn[pl.ds(T + BLK, BLK), :] = jnp.zeros((BLK, kvw), BF16)
            vt[:, pl.ds(T + BLK, BLK)] = jnp.zeros((kvw, BLK), BF16)

        @pl.when(has_prev)
        def _():
            k_dn.wait_send()
            v_dn.wait_send()
            k_up.wait_recv()
            v_up.wait_recv()

        @pl.when(jnp.logical_not(has_prev))
        def _():
            kn[pl.ds(0, BLK), :] = jnp.zeros((BLK, kvw), BF16)
            vt[:, pl.ds(0, BLK)] = jnp.zeros((kvw, BLK), BF16)

    key_w = 3 * BLK
    ones = jnp.ones((16, key_w), BF16)
    sinks = sink[...] * LOG2E
    pairs = qw // HEAD // 2

    def attend_pair(b, p):
        def run():
            s_all = mm(kn[b * BLK : b * BLK + key_w, :], qt[b, :, 2 * p * BLK : 2 * (p + 1) * BLK])
            yield
            lo, hi = bias_m[0], bias_m[1]
            if b == 0:
                lo = lo + jnp.where(idx == 0, NEG, 0.0)
            if b == nb - 1:
                hi = hi + jnp.where(idx == n_sp - 1, NEG, 0.0)
            probs, adds = [], []
            for u in range(2):
                h = 2 * p + u
                s = s_all[:, u * BLK : (u + 1) * BLK]
                s = jnp.concatenate([s[0:BLK] + lo, s[BLK : 2 * BLK], s[2 * BLK :] + hi], axis=0)
                sk = jnp.broadcast_to(sinks[:, h : h + 1], (1, BLK))
                m = jnp.maximum(jnp.max(s, axis=0, keepdims=True), sk)
                probs.append(jnp.exp2(s - m).astype(BF16))
                adds.append(jnp.exp2(sk - m))
            yield
            g = 2 * p // q_per
            vals = jnp.concatenate([vt[g * HEAD : (g + 1) * HEAD, b * BLK : b * BLK + key_w], ones], axis=0)
            o = mm(vals, jnp.concatenate(probs, axis=1))
            yield
            outs = []
            for u in range(2):
                cols = slice(u * BLK, (u + 1) * BLK)
                inv = 1.0 / (o[HEAD : HEAD + 1, cols] + adds[u])
                outs.append(o[0:HEAD, cols] * inv)
            z[b * BLK : (b + 1) * BLK, p * LANE : (p + 1) * LANE] = (
                jnp.concatenate(outs, axis=0).T.astype(BF16)
            )
        return run

    seq = []
    for n, i in enumerate(visit):
        if n > 0:
            seq.append(action(functools.partial(maybe_hop, n)))
        if i == 0:
            seq.append(action(kv_halo))
        todo = [attend_pair(i * per + u, p) for u in range(per) for p in range(pairs)]
        hosted = q_units(visit[n + 1]) if n + 1 < nchunk else []
        seq += blend(todo[:-3], hosted) + todo[-3:]
    with jax.named_scope("attend"):
        pipeline(seq)
    maybe_hop(nchunk)

    envs = {}

    def mix_begin(b):
        def run():
            env = envs[b] = {}
            c = ct[b]
            step = st[b]
            e = c - jnp.log2(jnp.maximum(step, 1e-37))
            cols = [v.astype(F32) for v in pieces(e)] + [jnp.ones((3 * hd2, LANE), F32)]
            cols += [jnp.zeros((LANE - 6 * hd2, LANE), F32)]
            env["lhs"] = jnp.concatenate(cols, axis=0).T.astype(BF16)
            env["c"] = [v.astype(F32) for v in pieces(c)]
            env["both"] = jnp.log2(jnp.maximum(step[0:heads] + step[heads:], 1e-37))
            rows = slice(b * BLK, (b + 1) * BLK)
            for g in range(groups):
                bm = bc[rows, g * STATE : (g + 1) * STATE]
                cm = bc[rows, state_w + g * STATE : state_w + (g + 1) * STATE]
                env[g] = mm_t(bm, cm)
        return run

    hrow = lax.broadcasted_iota(jnp.int32, (hd2, BLK), 0)

    def mix_diff(b, h):
        def run():
            env = envs[b]
            parts = []
            for r in (h, heads + h):
                own = hrow == r
                minus = jnp.where(own, -1.0, 0.0).astype(F32)
                rhs = [minus] * 3 + [jnp.where(own, v, 0.0) for v in env["c"]]
                rhs += [jnp.zeros((LANE - 6 * hd2, BLK), F32)]
                parts.append(jnp.concatenate(rhs, axis=0).astype(BF16))
            env["d", h] = mm(env["lhs"], jnp.concatenate(parts, axis=1))
        return run

    def mix_head(b, h):
        def run():
            env = envs[b]
            d = env.pop(("d", h))
            arg = jnp.where(ri < ci, d[:, 0:BLK], d[:, BLK:])
            arg = jnp.where(ri == ci, spread(env["both"], h, BLK), arg)
            weights = (env[h // per_group] * jnp.exp2(arg)).astype(BF16)
            yield
            y = mm(xt[b, h * HEAD : (h + 1) * HEAD, :], weights)
            yield
            ys[b, h * HEAD : (h + 1) * HEAD, :] = y
        return run

    heads_of = [(b, h) for b in range(nb) for h in range(heads)]
    ahead = 2
    seq = [mix_begin(0)] + [mix_diff(*heads_of[n]) for n in range(ahead)]
    todo = []
    for n, (b, h) in enumerate(heads_of):
        if h == heads // 2 and b + 1 < nb:
            todo.append(mix_begin(b + 1))
        if n + ahead < len(heads_of):
            todo.append(mix_diff(*heads_of[n + ahead]))
        todo.append(mix_head(b, h))
    seq += blend(todo, [u for i in range(nchunk) for u in gate_units(i)])
    with jax.named_scope("mix1"):
        pipeline(seq)

    with jax.named_scope("w_chain"):
        for d in range(2):
            @pl.when(targets[d])
            def _(d=d):
                for c in hops[d]:
                    c.wait_send()

            @pl.when(sources[d] & jnp.logical_not(targets[d]))
            def _(d=d):
                for c in hops[d]:
                    c.wait_recv()

    for d in range(2):
        order = list(range(nb)) if d == 0 else list(range(nb - 1, -1, -1))
        for h in range(heads):
            rows = slice(h * HEAD, (h + 1) * HEAD)
            total = jnp.where(sources[d], chain_r[d, rows, :].astype(F32), start[d, rows, :])
            for b in order:
                sb[b, d, rows, :] = total.astype(BF16)
                if b != order[-1]:
                    total = total * spread(dec[b], d * heads + h, HEAD) + gs[b, d, rows, :]

    def mix_close(k, u, g):
        b = chunk_base(k) // BLK + u
        part = slice(u * BLK, (u + 1) * BLK)

        def run():
            rows = pl.ds(pl.multiple_of(b * BLK, BLK), BLK)
            cm = bc[rows, state_w + g * STATE : state_w + (g + 1) * STATE]
            states = jnp.concatenate(
                [sb[b, d, g * gwid : (g + 1) * gwid, :] for d in range(2)], axis=0
            )
            carried = mm_t(states, cm)
            yield
            grow = jnp.exp2(ct[b])
            gated = []
            for u in range(per_group):
                h = g * per_group + u
                y = ys[b, h * HEAD : (h + 1) * HEAD, :]
                y = y + carried[u * HEAD : (u + 1) * HEAD] * spread(grow, h, HEAD)
                y = y + carried[gwid + u * HEAD : gwid + (u + 1) * HEAD] * spread(grow, heads + h, HEAD)
                gated.append(y * gt[b, h * HEAD : (h + 1) * HEAD, :])
            total = sum(jnp.sum(v * v, axis=0, keepdims=True) for v in gated)
            inv = lax.rsqrt(total * (1.0 / gwid) + epsilon)
            for t in range(per_group // 2):
                s = g * gwid + t * LANE
                v = jnp.concatenate([gated[2 * t], gated[2 * t + 1]], axis=0)
                zs[k][part, s : s + LANE] = (v * inv * ggt[s : s + LANE, :]).T.astype(BF16)
        return run

    for c in oc[:2]:
        c.wait()
    half_rows = T // 2
    steps = half_rows // ROWS
    width = wo.shape[1]
    cut = 2
    wide = width // cut
    copies = [
        [
            pltpu.make_async_remote_copy(
                src_ref=psend.at[pl.ds(i * ROWS, ROWS), pl.ds(j * wide, wide)],
                dst_ref=precv.at[pl.ds(i * ROWS, ROWS), pl.ds(j * wide, wide)],
                send_sem=sem_ps.at[cut * i + j],
                recv_sem=sem_pr.at[cut * i + j],
                device_id={"tp": peer},
                device_id_type=MESH,
            )
            for j in range(cut)
        ]
        for i in range(steps)
    ]

    def chunk_base(k):
        owner = peer if k < steps else me
        return owner * half_rows + (k % steps) * ROWS

    def out_units(k):
        zr = pl.ds(pl.multiple_of(chunk_base(k), ROWS), ROWS)
        i = k % steps
        dst = slice(i * ROWS, (i + 1) * ROWS)

        def unit(s):
            def run():
                part = mm(jnp.concatenate([z[zr, :], zs[k][...]], axis=1), wo[:, s : s + 256])
                yield
                if k < steps:
                    psend[dst, s : s + 256] = part.astype(BF16)
                else:
                    outv[dst, s : s + 256] = (
                        rounded(part) + precv[dst, s : s + 256].astype(F32)
                    ).astype(BF16)
            return run

        return [unit(s) for s in range(0, width, 256)]

    total_chunks = 2 * steps
    seq = []
    for k in range(total_chunks + 1):
        hosted = out_units(k - 1) if k > 0 else []
        main = []
        if k < total_chunks:
            for u in range(per):
                for g in range(groups):
                    main.append(mix_close(k, u, g))
        apart = len(hosted) // cut
        units = list(hosted)
        for j in range(cut - 1, -1, -1):
            if k > steps:
                units.insert(j * apart, action(copies[k - 1 - steps][j].wait))
            elif k > 0 and j > 0:
                units.insert(j * apart + 1, action(copies[k - 1][j - 1].start))
        if 1 < k <= steps + 1:
            units.insert(2 if k > steps else 1, action(copies[k - 2][cut - 1].start))
        seq += blend(units, main) if units else main
    with jax.named_scope("mix2"):
        pipeline(seq)


def tables(tokens, count):
    half = HEAD // 2
    frequency = rotary_base ** (-np.arange(half, dtype=np.float64) / half)
    inner = frequency[:, None] * np.arange(tokens, dtype=np.float64)[None, :]
    outer = np.arange(count, dtype=np.float64)[:, None] * tokens * frequency[None, :]
    outer = np.broadcast_to(outer[:, :, None], (count, half, LANE))
    return [f(a).astype(np.float32) for a in (inner, outer) for f in (np.cos, np.sin)]


def local(
    n_sp,
    inputs, mix_gain, w_query, w_key, w_value, query_gain, key_gain, sink_logit,
    w_inner, w_bmat, w_cmat, w_gate, w_step, conv_inner, conv_bmat, conv_cmat,
    step_bias, decay_rate, decay_offset, start_state, group_gain, w_out_attn, w_out_state,
):
    T, half = inputs.shape
    depth = w_query.shape[0]
    heads = w_step.shape[2]
    inner_w = w_inner.shape[1]
    state_w = w_bmat.shape[1]
    xw = inner_w + 2 * state_w
    kvw = w_key.shape[1]
    qw = w_query.shape[1]
    gw = w_gate.shape[1]
    width = w_out_attn.shape[1]
    nb = T // BLK
    nchunk = T // ROWS
    groups = state_w // STATE

    ws = jnp.transpose(w_step, (1, 2, 0)).reshape(2 * heads, depth)
    offs = jnp.transpose(decay_offset, (1, 2, 0)).reshape(2 * heads, T)
    start = start_state.reshape(2, inner_w, STATE)
    ct, sn, co, so = tables(T, n_sp)
    tri = np.triu(np.ones((BLK, BLK), np.float32))
    tri = np.concatenate([tri, tri.T], axis=1)
    any_spec = pl.BlockSpec(memory_space=pl.ANY)
    vm = pl.BlockSpec(memory_space=pltpu.VMEM)
    wcols = 2 * kvw + xw + qw + gw
    V = pltpu.VMEM
    dma = pltpu.SemaphoreType.DMA
    steps = T // 2 // ROWS
    hd2 = 2 * heads
    small = [
        ws, mix_gain.reshape(1, -1), query_gain.reshape(1, -1), key_gain.reshape(1, -1),
        sink_logit.reshape(1, -1), conv_inner, conv_bmat, conv_cmat, step_bias, decay_rate,
        offs, group_gain.reshape(1, -1), jnp.asarray(ct), jnp.asarray(sn), jnp.asarray(co),
        jnp.asarray(so), jnp.asarray(tri, dtype=BF16),
    ]
    scratch = [V(a.shape, a.dtype) for a in small] + [
        V((depth, wcols), BF16), V((LANE, depth), BF16),
        V((w_out_attn.shape[0] + w_out_state.shape[0], width), BF16),
        V((2, inner_w, STATE), F32),
        V((T, half), BF16), V((T, half), BF16), V((T, half), BF16), V((T, half), BF16), V((T, LANE), F32),
        V((2, nb, 2 * HEAD, LANE), F32),
        V((T + 2 * BLK, kvw), BF16), V((kvw, T + 2 * BLK), BF16),
        V((xw // LANE, T + 2 * EDGE, LANE), F32),
        V((nb, kvw, qw // HEAD * BLK), BF16), V((nb, gw, BLK), F32),
        V((T, 2 * state_w), BF16), V((nb, inner_w, BLK), BF16),
        V((nb, hd2, BLK), F32), V((nb, hd2, BLK), F32), V((nb, hd2, BLK), F32), V((nb, hd2, BLK), F32),
        V((inner_w, LANE), F32), V((2, BLK, BLK), F32),
        V((nb, 2, inner_w, STATE), F32), V((2, inner_w, STATE), F32), V((hd2, LANE), F32),
        V((nb, 2, inner_w, STATE), BF16), V((nb, inner_w, BLK), F32),
        V((T, qw), BF16), *[V((ROWS, inner_w), BF16) for _ in range(4)],
        V((T // 2, width), BF16), V((T // 2, width), BF16),
        V((2, xw // LANE, EDGE, LANE), F32),
        V((2, inner_w, STATE), BF16), V((2, inner_w, STATE), BF16),
        dma((len(small),)), dma((17,)), dma((nchunk,)), dma((nchunk,)), dma((nchunk,)),
        dma((6,)), dma((6,)), dma((2 * groups,)), dma((2 * groups,)), dma((2 * steps,)), dma((2 * steps,)),
    ]
    return pl.pallas_call(
        functools.partial(kernel, n_sp=n_sp),
        out_shape=pltpu.VMEM((T // 2, width), BF16),
        in_specs=[any_spec] * (11 + len(small)),
        out_specs=vm,
        scratch_shapes=scratch,
        compiler_params=pltpu.CompilerParams(
            collective_id=0, has_side_effects=True, vmem_limit_bytes=58720256
        ),
        name="mixer",
    )(
        inputs, w_query, w_key, w_value, w_inner, w_bmat, w_cmat, w_gate,
        w_out_attn, w_out_state, start, *small,
    )


def solution(mesh):
    return jax.shard_map(
        functools.partial(local, mesh.shape["sp"]),
        mesh=mesh,
        in_specs=(
            P(("fs", "sp"), "tp"),
            P(),
            P(None, "tp"),
            P(None, "tp"),
            P(None, "tp"),
            P(),
            P(),
            P("tp"),
            P(None, "tp"),
            P(None, "tp"),
            P(None, "tp"),
            P(None, "tp"),
            P(None, None, "tp"),
            P(None, "tp"),
            P(None, "tp"),
            P(None, "tp"),
            P(None, "tp"),
            P(None, "tp"),
            P("sp", None, "tp"),
            P("fs", "tp", None, None),
            P("tp"),
            P("tp", None),
            P("tp", None),
        ),
        out_specs=P(("fs", "sp", "tp"), None),
        check_vma=False,
    )
```
